512 devices in a mesh: sp: 128 (over z, x, core), tp: 4 (over y).
Axes of the slice: x: 4, y: 4, z: 16, core: 2. Of those that a mesh axis runs over, the one named last changes fastest.
Arguments:
- tokens: bfloat16 [65536, 2048], P(('sp', 'tp')), may hold values from -6 to 6
- norm_gain: float32 [2048], replicated, may hold values from 0.1 to 1.9
- pool_in_weight: bfloat16 [2048, 1024], P('sp', 'tp'), may hold values from -0.125 to 0.125
- query_weight: bfloat16 [2048, 1024], P('sp', 'tp'), may hold values from -0.125 to 0.125
- forget_weight: bfloat16 [2048, 1024], P('sp', 'tp'), may hold values from -0.125 to 0.125
- input_weight: bfloat16 [2048, 1024], P('sp', 'tp'), may hold values from -0.125 to 0.125
- forget_gap: float32 [1024], P('tp'), may hold values from 0 to 0.02
- decay_shift: float32 [8, 65536], P('tp', 'sp'), may hold values from -0.42 to 0
- out_gain: float32 [128], replicated, may hold values from 0.1 to 1.9
- pool_out_weight: bfloat16 [1024, 2048], P('tp', 'sp'), may hold values from -0.53033009 to 0.53033009
- recur_out_weight: bfloat16 [1024, 2048], P('tp', 'sp'), may hold values from -0.53033009 to 0.53033009
Outputs:
- mixed_out: bfloat16 [65536, 2048], P(('sp', 'tp'))
The draws below stay inside these ranges and needn't reach their ends.
All inputs are finite; a program needn't handle non-finite values.
Results may differ from the reference program's by a relative error of at most 0.014.
Values may be sent and summed in bfloat16 or wider, within the bound.
No kernel may reach another device: no remote copies, remote signals or barrier semaphores. Data moves between devices by JAX's collectives and lax.ppermute only.
A program may use at most 64 MiB of HBM per device.

```python
import jax
import jax.numpy as jnp
from jax import lax

D = 2048
GROUPS = 4
GC = 256
POOL = 1024
REC_HEADS = 8
RDIM = 128
REC = 1024
SPAN = 64
TOK_DEV = 512
SEQ = 65536
N_SP = 128
N_TP = 4


def slow_heads(key):
    order = jax.random.permutation(jax.random.fold_in(key, 11), REC_HEADS)
    return order < REC_HEADS // 2


def draw_forget_gap(key, part):
    slow_decay = slow_heads(key)
    unit = jax.random.uniform(jax.random.fold_in(key, 12), (REC_HEADS, RDIM), jnp.float32)
    slow_gap = jnp.exp(jnp.log(0.2) + unit * jnp.log(5.0)) / SEQ
    fast_gap = jnp.exp(jnp.log(0.01) + unit * jnp.log(2.0))
    gap_values = jnp.where(slow_decay[:, None], slow_gap, fast_gap)
    return gap_values.reshape(REC_HEADS * RDIM).astype(jnp.float32)


def draw_decay_shift(key, part):
    slow_decay = slow_heads(key)
    block_count = SEQ // TOK_DEV
    unit = jax.random.uniform(jax.random.fold_in(key, 13), (REC_HEADS, block_count), jnp.float32)
    slow_rate = jnp.exp(jnp.log(0.1) + unit * jnp.log(5.0)) / SEQ
    fast_rate = jnp.exp(jnp.log(0.005) + unit * jnp.log(3.0))
    rates = jnp.where(slow_decay[:, None], slow_rate, fast_rate)
    drawn_result = -jnp.repeat(rates, TOK_DEV, axis=1)
    third = SEQ // 3
    offsets = jax.random.randint(jax.random.fold_in(key, 14), (REC_HEADS, 3), 0, third)
    spots = offsets + jnp.arange(3, dtype=jnp.int32)[None, :] * third
    depth = jax.random.uniform(jax.random.fold_in(key, 15), (REC_HEADS, 3), jnp.float32, 0.22, 0.4)
    places = jnp.arange(SEQ, dtype=jnp.int32)
    match_count = (places[None, None, :] == spots[:, :, None]).astype(jnp.float32) * depth[:, :, None]
    spike_events = jnp.sum(match_count, axis=1) * slow_decay[:, None].astype(jnp.float32)
    return (drawn_result - spike_events).astype(jnp.float32)


def heavy_columns(key, rows, salt):
    chosen = jax.random.randint(jax.random.fold_in(key, 21), (), 0, N_SP)
    block_width = D // N_SP
    column_block = jnp.arange(D, dtype=jnp.int32) // block_width
    factor = jnp.where(column_block == chosen, 4.0, 1.0).astype(jnp.float32)
    scale = (POOL + REC) ** (-0.5)
    drawn = jnp.clip(jax.random.normal(jax.random.fold_in(key, salt), (rows, D), jnp.float32), -6.0, 6.0)
    return (drawn * factor[None, :] * scale).astype(jnp.float32)


def draw_pool_out_weight(key, part):
    return heavy_columns(key, POOL, 22).astype(jnp.bfloat16)


def draw_recur_out_weight(key, part):
    return heavy_columns(key, REC, 23).astype(jnp.bfloat16)


def shard_levels(key, dims, pieces, least, top_value):
    gain, own = 1.0, jax.random.fold_in(key, 6)
    for axis_at, parts in pieces:
        heights = jnp.exp(jax.random.uniform(jax.random.fold_in(own, axis_at), (parts,), jnp.float32, least / len(pieces), top_value / len(pieces)))
        gain = gain * jnp.repeat(heights, dims[axis_at] // parts).reshape([-1 if axis == axis_at else 1 for axis in range(len(dims))])
    return gain


def noise(own_key, shape, scale, bound, cuts=(), kind=jnp.bfloat16):
    level = shard_levels(own_key, shape, cuts, -0.22, 0.18) if cuts else 1.0
    values = jax.random.normal(own_key, shape, jnp.float32) * scale * level
    return jnp.minimum(jnp.maximum(values, -bound), bound).astype(kind)


def setup_inputs(seed: int = 0) -> dict:
    seeds = jax.random.split(jax.random.key(seed), 12)
    return {
        "tokens": noise(seeds[0], (SEQ, D), 1.0, 6.0, ((0, 512),)),
        "norm_gain": jnp.clip(1.0 + 0.18 * jax.random.normal(seeds[1], (D,), jnp.float32), 0.1, 1.9),
        "pool_in_weight": noise(seeds[2], (D, POOL), D ** -0.5, 0.125, ((0, 128), (1, 4))),
        "query_weight": noise(seeds[3], (D, REC), D ** -0.5, 0.125, ((0, 128), (1, 4))),
        "forget_weight": noise(seeds[4], (D, REC), D ** -0.5, 0.125, ((0, 128), (1, 4))),
        "input_weight": noise(seeds[5], (D, REC), D ** -0.5, 0.125, ((0, 128), (1, 4))),
        "forget_gap": draw_forget_gap(jax.random.fold_in(seeds[11], 71), 0),
        "decay_shift": draw_decay_shift(jax.random.fold_in(seeds[11], 71), 0),
        "out_gain": jnp.clip(1.0 + 0.18 * jax.random.normal(seeds[8], (RDIM,), jnp.float32), 0.1, 1.9),
        "pool_out_weight": draw_pool_out_weight(jax.random.fold_in(seeds[11], 71), 0),
        "recur_out_weight": draw_recur_out_weight(jax.random.fold_in(seeds[11], 71), 0),
    }


EPSILON = 1e-06
EXACT_MATMUL = lax.Precision.HIGHEST

def pooling(pooled_in):
    length = pooled_in.shape[0]
    groups = pooled_in.astype(jnp.float32).reshape(length, GROUPS, GC)
    running = jnp.cumsum(groups, axis=0)
    counter = jnp.arange(1, length + 1, dtype=jnp.float32)[:, None]
    means = []
    for index in range(GROUPS):
        width = 2 ** (index + 1)
        current = running[:, index]
        lagged = jnp.pad(current[:length - width], ((width, 0), (0, 0)))
        means.append((current - lagged) / jnp.minimum(counter, jnp.float32(width)))
    mixed = jnp.stack(means, axis=1) - groups
    return mixed.astype(jnp.bfloat16).reshape(length, GROUPS * GC)

def recurrence(query, forget_pre, values, forget_gap, decay_shift, out_gain):
    length = query.shape[0]
    block_count = length // SPAN
    gate_pre = forget_pre.astype(jnp.float32).reshape(length, REC_HEADS, RDIM)
    opened = forget_gap.reshape(REC_HEADS, RDIM) * jax.nn.sigmoid(-gate_pre)
    log_decay = jnp.log1p(-opened) + decay_shift.T[:, :, None]

    def to_blocks(tensor):
        return tensor.reshape(block_count, SPAN, REC_HEADS, RDIM).transpose(0, 2, 1, 3)
    causal = jnp.tril(jnp.ones((SPAN, SPAN), jnp.bool_))

    def block_step(state_matrix, block):
        query_block, decay_block, key_tile_rows, value_tile_rows = block
        inner_block_output = jnp.cumsum(decay_block, axis=1)
        block_decay_total = inner_block_output[:, -1:, :]
        decayed_query = query_block * jnp.exp(inner_block_output)
        scores = jnp.einsum('htk,hsk->hts', decayed_query, key_tile_rows * jnp.exp(-inner_block_output), precision=EXACT_MATMUL)
        scores = jnp.where(causal, scores, 0.0)
        received_output = jnp.einsum('hts,hsv->htv', scores, value_tile_rows, precision=EXACT_MATMUL)
        received_output = received_output + jnp.einsum('dux,dxs->dus', decayed_query, state_matrix, precision=EXACT_MATMUL)
        growth_factor = jnp.einsum('xgb,xgi->xbi', key_tile_rows * jnp.exp(block_decay_total - inner_block_output), value_tile_rows, precision=EXACT_MATMUL)
        new_state = jnp.exp(block_decay_total[:, 0, :])[:, :, None] * state_matrix + growth_factor
        return (new_state, received_output)
    start_state = jnp.zeros((REC_HEADS, RDIM, RDIM), jnp.float32)
    inputs = (to_blocks(query.astype(jnp.float32)), to_blocks(log_decay), to_blocks(opened), to_blocks(values.astype(jnp.float32)))
    _, received_output = lax.scan(block_step, start_state, inputs)
    received_output = received_output.transpose(0, 2, 1, 3).reshape(length, REC_HEADS, RDIM)
    spread = lax.rsqrt(lax.optimization_barrier(jnp.mean(received_output * received_output, axis=-1, keepdims=True)) + EPSILON)
    normed = received_output * spread * out_gain
    return normed.astype(jnp.bfloat16).reshape(length, REC_HEADS * RDIM)

def reference(tokens, norm_gain, pool_in_weight, query_weight, forget_weight, input_weight, forget_gap, decay_shift, out_gain, pool_out_weight, recur_out_weight):
    floats = tokens.astype(jnp.float32)
    scale = lax.rsqrt(lax.optimization_barrier(jnp.mean(floats * floats, axis=-1, keepdims=True)) + EPSILON)
    normed = (floats * scale * norm_gain).astype(jnp.bfloat16)
    pooled_in = jnp.dot(normed, pool_in_weight, preferred_element_type=jnp.float32).astype(jnp.bfloat16)
    query = jnp.dot(normed, query_weight, preferred_element_type=jnp.float32).astype(jnp.bfloat16)
    forget_pre = jnp.dot(normed, forget_weight, preferred_element_type=jnp.float32).astype(jnp.bfloat16)
    values = jnp.dot(normed, input_weight, preferred_element_type=jnp.float32).astype(jnp.bfloat16)
    pool_mixed = pooling(pooled_in)
    recur_mixed = recurrence(query, forget_pre, values, forget_gap, decay_shift, out_gain)
    pool_share = GROUPS * GC // N_TP
    recur_share = REC_HEADS * RDIM // N_TP
    total = jnp.zeros((tokens.shape[0], D), jnp.float32)
    for index in range(N_TP):
        part = jnp.dot(pool_mixed[:, index * pool_share:(index + 1) * pool_share], pool_out_weight[index * pool_share:(index + 1) * pool_share], preferred_element_type=jnp.float32)
        part = part + jnp.dot(recur_mixed[:, index * recur_share:(index + 1) * recur_share], recur_out_weight[index * recur_share:(index + 1) * recur_share], preferred_element_type=jnp.float32)
        part = lax.optimization_barrier(part.astype(jnp.bfloat16))
        total = total + part.astype(jnp.float32)
    return total.astype(jnp.bfloat16)
```

```python
import jax
import jax.numpy as jnp
from jax import lax
from jax.experimental import pallas as pl
from jax.experimental.pallas import tpu as pltpu
from jax.sharding import Mesh
from jax.sharding import PartitionSpec as P


GROUPS = 4
RDIM = 128
CHUNK = 128
RIM = 16
SP = ("sp_0", "sp_1", "sp_2")
SP_TP = ("sp_0", "sp_1", "sp_2", "tp")
EPSILON = 1e-06
BF = jnp.bfloat16
F32 = jnp.float32
NT = (((1,), (1,)), ((), ()))
TN = (((0,), (0,)), ((), ()))
NN = (((1,), (0,)), ((), ()))


def dot(a, b, dims=NN):
    return lax.dot_general(a, b, dims, preferred_element_type=F32)


def halves(x):
    high = x.astype(BF)
    return high, (x - high.astype(F32)).astype(BF)


def dot_wide(a, b, dims=NN):
    ah, al = halves(a)
    bh, bl = halves(b)
    return dot(ah, bh, dims) + (dot(ah, bl, dims) + dot(al, bh, dims))


def dot_left(a, b, dims=NN):
    ah, al = halves(a)
    return dot(ah, b, dims) + dot(al, b, dims)


def sent_to_all(x, axis):
    copies = jnp.broadcast_to(x, (lax.axis_size(axis), *x.shape))
    return lax.all_to_all(copies, axis, split_axis=0, concat_axis=0, tiled=True)


def ring_gather(x, axis):
    n = lax.axis_size(axis)
    up = [(i, (i + 1) % n) for i in range(n)]
    down = [(i, (i - 1) % n) for i in range(n)]
    half = x.shape[0] // 2
    before = lax.ppermute(x, axis, up)
    after = lax.ppermute(x, axis, down)
    far_low = lax.ppermute(before[:half], axis, up)
    far_high = lax.ppermute(after[half:], axis, down)
    return x, before, after, far_low, far_high


def places(index, n):
    return [index, lax.rem(index + n - 1, n), lax.rem(index + 1, n), lax.rem(index + 2, n)]


def assemble(info_ref, mine_ref, other_ref, whole_ref):
    core = info_ref[0]
    nx, nz, rows, _ = mine_ref.shape
    spots = places(info_ref[3], nx)

    def put(z, carry):
        for k, spot in enumerate(spots):
            at = ((z * nx + spot) * 2) * rows
            here = pl.ds(pl.multiple_of(at + core * rows, rows), rows)
            there = pl.ds(pl.multiple_of(at + (1 - core) * rows, rows), rows)
            whole_ref[here, :] = mine_ref[k, z]
            whole_ref[there, :] = other_ref[k, z]
        return carry

    lax.fori_loop(0, nz, put, 0)


def state_kernel(
    info_ref,
    own_ref,
    before_ref,
    after_ref,
    low_ref,
    high_ref,
    gain_ref,
    mine_ref,
    other_ref,
    gap_ref,
    shift_ref,
    normed_ref,
    values_ref,
    opened_ref,
    cum_ref,
    growth_ref,
    payload_ref,
    whole_ref,
    both_ref,
):
    rows, _ = normed_ref.shape
    cols = gap_ref.shape[1]
    assemble(info_ref, mine_ref, other_ref, whole_ref)
    block = own_ref.shape[0]
    own, before, after, far = places(info_ref[1], rows // block)

    def norm(from_ref, start, i):
        floats = from_ref[pl.ds(pl.multiple_of(i * 32, 32), 32), :].astype(F32)
        scale = lax.rsqrt(jnp.mean(floats * floats, axis=-1, keepdims=True) + EPSILON)
        at = pl.ds(pl.multiple_of(start + i * 32, 32), 32)
        normed_ref[at, :] = (floats * scale * gain_ref[...]).astype(BF)

    def norm_all(i, carry):
        for from_ref, place in ((own_ref, own), (before_ref, before), (after_ref, after)):
            norm(from_ref, place * block, i)
        return carry

    def norm_far(i, carry):
        norm(low_ref, far * block, i)
        norm(high_ref, far * block + block // 2, i)
        return carry

    lax.fori_loop(0, block // 32, norm_all, 0)
    lax.fori_loop(0, block // 64, norm_far, 0)
    both_ref[...] = dot(normed_ref[...], whole_ref[...])
    row = lax.broadcasted_iota(jnp.int32, (CHUNK, CHUNK), 0)
    col = lax.broadcasted_iota(jnp.int32, (CHUNK, CHUNK), 1)
    tril = (row >= col).astype(BF)
    heads = cols // RDIM
    for h in range(heads):
        lanes = slice(h * RDIM, (h + 1) * RDIM)
        state = jnp.zeros((RDIM, RDIM), F32)
        faded = jnp.zeros((1, RDIM), F32)
        for c in range(rows // CHUNK):
            at = slice(c * CHUNK, (c + 1) * CHUNK)
            pre = both_ref[at, lanes].astype(BF).astype(F32)
            values = both_ref[at, cols + h * RDIM : cols + (h + 1) * RDIM].astype(BF)
            opened = gap_ref[:, lanes] / (1.0 + jnp.exp(pre))
            decay = jnp.log1p(-opened) + shift_ref[at, h : h + 1]
            d0, d1 = halves(decay)
            d2 = (decay - d0.astype(F32) - d1.astype(F32)).astype(BF)
            cum = dot(tril, d0) + (dot(tril, d1) + dot(tril, d2))
            total = cum[CHUNK - 1 :, :]
            growth = dot_left_t(values, opened * jnp.exp(total - cum))
            values_ref[at, lanes] = values
            opened_ref[at, lanes] = opened
            cum_ref[at, lanes] = cum
            growth_ref[c, :, lanes] = growth
            state = state * jnp.exp(total) + growth
            faded = faded + total
        payload_ref[:, lanes] = state
        payload_ref[:, cols + h * RDIM : cols + (h + 1) * RDIM] = jnp.broadcast_to(faded, (RDIM, RDIM))


def dot_left_t(values, key):
    kh, kl = halves(key)
    return dot(values, kh, TN) + dot(values, kl, TN)


def scan_kernel(got_ref, start_ref):
    rows, cols = start_ref.shape
    per = rows // lax.axis_size(SP)
    state = got_ref[:, :cols]
    fade = jnp.exp(got_ref[:, cols:])
    index = lax.broadcasted_iota(jnp.int32, (rows, cols), 0)
    step = per
    while step < rows:
        inside = index >= step
        before = jnp.where(inside, pltpu.roll(state, step, 0), 0.0)
        earlier = jnp.where(inside, pltpu.roll(fade, step, 0), 1.0)
        state = fade * before + state
        fade = fade * earlier
        step *= 2
    start_ref[...] = jnp.where(index >= per, pltpu.roll(state, per, 0), 0.0)


def inner_kernel(
    info_ref,
    normed_ref,
    mine_ref,
    other_ref,
    values_ref,
    opened_ref,
    cum_ref,
    pooled_ref,
    decayed_ref,
    heard_ref,
    whole_ref,
    both_ref,
):
    rows, cols = values_ref.shape
    assemble(info_ref, mine_ref, other_ref, whole_ref)
    both_ref[...] = dot(normed_ref[...], whole_ref[...])
    pooled_ref[...] = both_ref[:, cols:].astype(BF)
    row = lax.broadcasted_iota(jnp.int32, (CHUNK, CHUNK), 0)
    col = lax.broadcasted_iota(jnp.int32, (CHUNK, CHUNK), 1)
    for h in range(cols // RDIM):
        lanes = slice(h * RDIM, (h + 1) * RDIM)
        for c in range(rows // CHUNK):
            at = slice(c * CHUNK, (c + 1) * CHUNK)
            cum = cum_ref[at, lanes]
            query = both_ref[at, lanes].astype(BF).astype(F32) * jnp.exp(cum)
            key = opened_ref[at, lanes] * jnp.exp(-cum)
            scores = jnp.where(row >= col, dot_wide(query, key, NT), 0.0)
            decayed_ref[at, lanes] = query
            heard_ref[at, lanes] = dot_left(scores, values_ref[at, lanes])


def final_kernel(
    info_ref,
    start_ref,
    growth_ref,
    cum_ref,
    decayed_ref,
    heard_ref,
    pooled_ref,
    rim_ref,
    gain_ref,
    mine_ref,
    other_ref,
    part_ref,
    whole_ref,
    mixed_ref,
):
    rows, cols = cum_ref.shape
    assemble(info_ref, mine_ref, other_ref, whole_ref)
    group = info_ref[1]
    padded = jnp.concatenate([rim_ref[...], pooled_ref[...]], axis=0).astype(F32)
    running = padded
    chosen = None
    for level in range(GROUPS):
        running = running + pltpu.roll(running, 2**level, 0)
        chosen = running if chosen is None else jnp.where(group == level, running, chosen)
    width = jnp.left_shift(jnp.int32(2), group)
    position = info_ref[2] + lax.broadcasted_iota(jnp.int32, (rows, cols), 0)
    divisor = jnp.minimum(position + 1, width).astype(F32)
    mixed_ref[:, :cols] = (chosen[RIM:] / divisor - padded[RIM:]).astype(BF)
    for h in range(cols // RDIM):
        lanes = slice(h * RDIM, (h + 1) * RDIM)
        state = start_ref[:, lanes]
        for c in range(rows // CHUNK):
            at = slice(c * CHUNK, (c + 1) * CHUNK)
            heard = heard_ref[at, lanes] + dot_wide(decayed_ref[at, lanes], state, NT)
            spread = lax.rsqrt(jnp.mean(heard * heard, axis=-1, keepdims=True) + EPSILON)
            mixed_ref[at, cols + h * RDIM : cols + (h + 1) * RDIM] = (
                heard * spread * gain_ref[...]
            ).astype(BF)
            total = cum_ref[(c + 1) * CHUNK - 1 : (c + 1) * CHUNK, lanes]
            state = state * jnp.exp(total) + growth_ref[c, :, lanes]

    def out(i, carry):
        at = pl.ds(pl.multiple_of(i * 256, 256), 256)
        part_ref[:, at] = dot(mixed_ref[...], whole_ref[at, :], NT).astype(BF)
        return carry

    lax.fori_loop(0, part_ref.shape[1] // 256, out, 0)


VMEM = pl.BlockSpec(memory_space=pltpu.VMEM)
SMEM = pl.BlockSpec(memory_space=pltpu.SMEM)


def call(kernel, outs, scratch, flops, moved, *args):
    return pl.pallas_call(
        kernel,
        out_shape=outs,
        in_specs=[SMEM if a.dtype == jnp.int32 else VMEM for a in args],
        out_specs=jax.tree.map(lambda _: VMEM, outs),
        scratch_shapes=scratch,
        cost_estimate=pl.CostEstimate(flops=flops, bytes_accessed=moved, transcendentals=0),
    )(*args)


def shape(dims, dtype):
    return jax.ShapeDtypeStruct(dims, dtype)


def stacked(pieces):
    own, before, after, low, high = pieces
    far = jnp.concatenate([low, high], axis=0)
    return jnp.stack([own, before, after, far])


def over_cores(x):
    return lax.ppermute(x, "sp_2", [(0, 1), (1, 0)])


def layer(
    tokens,
    norm_gain,
    pool_in_weight,
    query_weight,
    forget_weight,
    input_weight,
    forget_gap,
    decay_shift,
    out_gain,
    pool_out_weight,
    recur_out_weight,
):
    width = tokens.shape[1]
    cols = query_weight.shape[1]
    tp = lax.axis_size("tp")
    rows = tokens.shape[0] * tp
    devices = lax.axis_size(SP)
    core = lax.axis_index("sp_2")
    group = lax.axis_index("tp")
    info = jnp.stack([core, group, lax.axis_index(SP) * rows, lax.axis_index("sp_1")]).astype(jnp.int32)

    pieces = ring_gather(tokens, "tp")
    first = jnp.concatenate([forget_weight, input_weight], axis=1)
    second = jnp.concatenate(
        [query_weight, pool_in_weight, pool_out_weight.T, recur_out_weight.T], axis=1
    )
    first_z = sent_to_all(first, "sp_0")
    second_z = sent_to_all(second, "sp_0")
    first_zx = stacked(ring_gather(first_z, "sp_1"))
    first_other = over_cores(first_zx)
    in_zx = stacked(ring_gather(second_z[..., : 2 * cols], "sp_1"))
    in_other = over_cores(in_zx)
    out_zx = stacked(ring_gather(second_z[..., 2 * cols :], "sp_1"))
    out_other = over_cores(out_zx)

    normed, values, opened, cum, growth, payload = call(
        state_kernel,
        [
            shape((rows, width), BF),
            shape((rows, cols), BF),
            shape((rows, cols), F32),
            shape((rows, cols), F32),
            shape((rows // CHUNK, RDIM, cols), F32),
            shape((RDIM, 2 * cols), F32),
        ],
        [pltpu.VMEM((width, 2 * cols), BF), pltpu.VMEM((rows, 2 * cols), F32)],
        4 * rows * width * cols,
        8 << 20,
        info,
        *pieces,
        norm_gain[None, :],
        first_zx,
        first_other,
        forget_gap[None, :],
        decay_shift.T,
    )

    got = lax.all_to_all(payload, SP, split_axis=0, concat_axis=0, tiled=True)
    start = call(scan_kernel, shape((RDIM, cols), F32), [], 1 << 22, 1 << 20, got)
    start = lax.all_to_all(start, SP, split_axis=0, concat_axis=0, tiled=True)
    pooled, decayed, heard = call(
        inner_kernel,
        [shape((rows, cols), BF), shape((rows, cols), F32), shape((rows, cols), F32)],
        [pltpu.VMEM((width, 2 * cols), BF), pltpu.VMEM((rows, 2 * cols), F32)],
        4 * rows * width * cols,
        8 << 20,
        info,
        normed,
        in_zx,
        in_other,
        values,
        opened,
        cum,
    )
    order = [(i - 1, i) for i in range(1, devices)]
    rim = lax.ppermute(pooled[rows - RIM :], SP, order)
    part = call(
        final_kernel,
        shape((rows, width), BF),
        [pltpu.VMEM((width, 2 * cols), BF), pltpu.VMEM((rows, 2 * cols), BF)],
        4 * rows * width * cols,
        8 << 20,
        info,
        start,
        growth,
        cum,
        decayed,
        heard,
        pooled,
        rim,
        out_gain[None, :],
        out_zx,
        out_other,
    )
    parts = lax.all_to_all(
        part.reshape(tp, rows // tp, width), "tp", split_axis=0, concat_axis=0, tiled=True
    )
    return jnp.sum(parts.astype(F32), axis=0).astype(BF)


def solution(mesh):
    split = Mesh(mesh.devices.reshape(16, 4, 2, mesh.shape["tp"]), ("sp_0", "sp_1", "sp_2", "tp"))
    in_specs = (
        P(SP_TP, None),
        P(),
        P(SP, "tp"),
        P(SP, "tp"),
        P(SP, "tp"),
        P(SP, "tp"),
        P("tp"),
        P("tp", SP),
        P(),
        P("tp", SP),
        P("tp", SP),
    )
    out_specs = P(SP_TP, None)
    return jax.shard_map(layer, mesh=split, in_specs=in_specs, out_specs=out_specs, check_vma=False)
```

```python
import jax
import jax.numpy as jnp
from jax import lax
from jax.experimental import pallas as pl
from jax.experimental.pallas import tpu as pltpu
from jax.sharding import Mesh
from jax.sharding import PartitionSpec as P


GROUPS = 4
RDIM = 128
CHUNK = 128
RIM = 16
FAR, NEAR, ACROSS, CORE = "sp_f", "sp_n", "sp_x", "sp_c"
DEPTH = (FAR, NEAR)
PLANE = (ACROSS, CORE)
SP = (FAR, NEAR, ACROSS, CORE)
SP_TP = (FAR, NEAR, ACROSS, CORE, "tp")
EPSILON = 1e-06
BF = jnp.bfloat16
F32 = jnp.float32
NT = (((1,), (1,)), ((), ()))
TN = (((0,), (0,)), ((), ()))
NN = (((1,), (0,)), ((), ()))


def dot(a, b, dims=NN):
    return lax.dot_general(a, b, dims, preferred_element_type=F32)


def halves(x):
    high = x.astype(BF)
    return high, (x - high.astype(F32)).astype(BF)


def dot_wide(a, b, dims=NN):
    ah, al = halves(a)
    bh, bl = halves(b)
    return dot(ah, bh, dims) + (dot(ah, bl, dims) + dot(al, bh, dims))


def dot_left(a, b, dims=NN):
    ah, al = halves(a)
    return dot(ah, b, dims) + dot(al, b, dims)


def sent_to_all(x, axis):
    copies = jnp.broadcast_to(x, (lax.axis_size(axis), *x.shape))
    return lax.all_to_all(copies, axis, split_axis=0, concat_axis=0, tiled=True)


def ring_gather(x, axis):
    n = lax.axis_size(axis)
    up = [(i, (i + 1) % n) for i in range(n)]
    down = [(i, (i - 1) % n) for i in range(n)]
    half = x.shape[0] // 2
    before = lax.ppermute(x, axis, up)
    after = lax.ppermute(x, axis, down)
    far_low = lax.ppermute(before[:half], axis, up)
    far_high = lax.ppermute(after[half:], axis, down)
    return x, before, after, far_low, far_high


def places(index, n):
    return [index, lax.rem(index + n - 1, n), lax.rem(index + 1, n), lax.rem(index + 2, n)]


def fetches(core, mine_ref, other_ref, lanes, whole_ref, sems):
    nx, near = mine_ref.shape[:2]
    copies = []
    for x in range(nx):
        for n in range(near):
            for side, from_ref in enumerate((mine_ref, other_ref)):
                to = core if side == 0 else 1 - core
                copies.append(
                    pltpu.make_async_copy(
                        from_ref.at[x, n, :, :, lanes],
                        whole_ref.at[:, n, x, to],
                        sems.at[len(copies)],
                    )
                )
    return copies


def started(copies):
    for copy in copies:
        copy.start()


def finished(copies):
    for copy in copies:
        copy.wait()


def state_kernel(
    info_ref,
    own_ref,
    before_ref,
    after_ref,
    low_ref,
    high_ref,
    gain_ref,
    mine_ref,
    other_ref,
    gap_ref,
    shift_ref,
    normed_ref,
    values_ref,
    opened_ref,
    cum_ref,
    growth_ref,
    payload_ref,
    whole_ref,
    sems,
    both_ref,
):
    rows, _ = normed_ref.shape
    cols = gap_ref.shape[1]
    copies = fetches(info_ref[0], mine_ref, other_ref, slice(0, 2 * cols), whole_ref, sems)
    started(copies)
    block = own_ref.shape[0]
    own, before, after, far = places(info_ref[1], rows // block)

    def norm(from_ref, start, i):
        floats = from_ref[pl.ds(pl.multiple_of(i * 32, 32), 32), :].astype(F32)
        scale = lax.rsqrt(jnp.mean(floats * floats, axis=-1, keepdims=True) + EPSILON)
        at = pl.ds(pl.multiple_of(start + i * 32, 32), 32)
        normed_ref[at, :] = (floats * scale * gain_ref[...]).astype(BF)

    def norm_all(i, carry):
        for from_ref, place in ((own_ref, own), (before_ref, before), (after_ref, after)):
            norm(from_ref, place * block, i)
        return carry

    def norm_far(i, carry):
        norm(low_ref, far * block, i)
        norm(high_ref, far * block + block // 2, i)
        return carry

    lax.fori_loop(0, block // 32, norm_all, 0)
    lax.fori_loop(0, block // 64, norm_far, 0)
    finished(copies)
    both_ref[...] = dot(normed_ref[...], whole_ref[...].reshape(-1, 2 * cols))
    row = lax.broadcasted_iota(jnp.int32, (CHUNK, CHUNK), 0)
    col = lax.broadcasted_iota(jnp.int32, (CHUNK, CHUNK), 1)
    tril = (row >= col).astype(BF)
    heads = cols // RDIM
    for h in range(heads):
        lanes = slice(h * RDIM, (h + 1) * RDIM)
        state = jnp.zeros((RDIM, RDIM), F32)
        faded = jnp.zeros((1, RDIM), F32)
        for c in range(rows // CHUNK):
            at = slice(c * CHUNK, (c + 1) * CHUNK)
            pre = both_ref[at, lanes].astype(BF).astype(F32)
            values = both_ref[at, cols + h * RDIM : cols + (h + 1) * RDIM].astype(BF)
            opened = gap_ref[:, lanes] / (1.0 + jnp.exp(pre))
            decay = jnp.log1p(-opened) + shift_ref[at, h : h + 1]
            d0, d1 = halves(decay)
            d2 = (decay - d0.astype(F32) - d1.astype(F32)).astype(BF)
            cum = dot(tril, d0) + (dot(tril, d1) + dot(tril, d2))
            total = cum[CHUNK - 1 :, :]
            growth = dot_left_t(values, opened * jnp.exp(total - cum))
            values_ref[at, lanes] = values
            opened_ref[at, lanes] = opened
            cum_ref[at, lanes] = cum
            growth_ref[c, :, lanes] = growth
            state = state * jnp.exp(total) + growth
            faded = faded + total
        payload_ref[:, lanes] = state
        payload_ref[:, cols + h * RDIM : cols + (h + 1) * RDIM] = jnp.broadcast_to(faded, (RDIM, RDIM))


def dot_left_t(values, key):
    kh, kl = halves(key)
    return dot(values, kh, TN) + dot(values, kl, TN)


def plane_kernel(got_ref, before_ref, faded_ref, total_ref):
    rows = got_ref.shape[1]
    cols = before_ref.shape[2]
    state = jnp.zeros((rows, cols), F32)
    faded = jnp.zeros((1, cols), F32)
    for d in range(got_ref.shape[0]):
        fade = got_ref[d, :1, cols:]
        before_ref[d] = state
        faded_ref[d : d + 1, :] = faded
        state = state * jnp.exp(fade) + got_ref[d, :, :cols]
        faded = faded + fade
    high = faded.astype(BF).astype(F32)
    row = lax.broadcasted_iota(jnp.int32, (16, cols), 0)
    total_ref[:rows, :] = state.astype(BF)
    total_ref[rows:, :] = jnp.where(row == 0, high, jnp.where(row == 1, faded - high, 0.0)).astype(BF)


def depth_kernel(info_ref, totals_ref, before_ref, faded_ref, start_ref):
    planes = totals_ref.shape[0]
    devices, rows, cols = before_ref.shape
    state = jnp.zeros((rows, cols), F32)
    for z in range(planes):
        got = totals_ref[z].astype(F32)
        fade = got[rows : rows + 1] + got[rows + 1 : rows + 2]
        state = jnp.where(z < info_ref[4], state * jnp.exp(fade) + got[:rows], state)
    for d in range(devices):
        start_ref[d] = before_ref[d] + jnp.exp(faded_ref[d : d + 1, :]) * state


def inner_kernel(
    info_ref,
    normed_ref,
    mine_ref,
    other_ref,
    values_ref,
    opened_ref,
    cum_ref,
    pooled_ref,
    decayed_ref,
    heard_ref,
    whole_ref,
    sems,
    both_ref,
):
    rows, cols = values_ref.shape
    copies = fetches(info_ref[0], mine_ref, other_ref, slice(2 * cols, 4 * cols), whole_ref, sems)
    started(copies)
    finished(copies)
    both_ref[...] = dot(normed_ref[...], whole_ref[...].reshape(-1, 2 * cols))
    pooled_ref[...] = both_ref[:, cols:].astype(BF)
    row = lax.broadcasted_iota(jnp.int32, (CHUNK, CHUNK), 0)
    col = lax.broadcasted_iota(jnp.int32, (CHUNK, CHUNK), 1)
    for h in range(cols // RDIM):
        lanes = slice(h * RDIM, (h + 1) * RDIM)
        for c in range(rows // CHUNK):
            at = slice(c * CHUNK, (c + 1) * CHUNK)
            cum = cum_ref[at, lanes]
            query = both_ref[at, lanes].astype(BF).astype(F32) * jnp.exp(cum)
            key = opened_ref[at, lanes] * jnp.exp(-cum)
            scores = jnp.where(row >= col, dot_wide(query, key, NT), 0.0)
            decayed_ref[at, lanes] = query
            heard_ref[at, lanes] = dot_left(scores, values_ref[at, lanes])


def final_kernel(
    info_ref,
    start_ref,
    growth_ref,
    cum_ref,
    decayed_ref,
    heard_ref,
    pooled_ref,
    rim_ref,
    gain_ref,
    mine_ref,
    other_ref,
    part_ref,
    whole_ref,
    sems,
    mixed_ref,
):
    rows, cols = cum_ref.shape
    copies = fetches(info_ref[0], mine_ref, other_ref, slice(0, 2 * cols), whole_ref, sems)
    started(copies)
    group = info_ref[1]
    padded = jnp.concatenate([rim_ref[...], pooled_ref[...]], axis=0).astype(F32)
    running = padded
    chosen = None
    for level in range(GROUPS):
        running = running + pltpu.roll(running, 2**level, 0)
        chosen = running if chosen is None else jnp.where(group == level, running, chosen)
    width = jnp.left_shift(jnp.int32(2), group)
    position = info_ref[2] + lax.broadcasted_iota(jnp.int32, (rows, cols), 0)
    divisor = jnp.minimum(position + 1, width).astype(F32)
    mixed_ref[:, :cols] = (chosen[RIM:] / divisor - padded[RIM:]).astype(BF)
    for h in range(cols // RDIM):
        lanes = slice(h * RDIM, (h + 1) * RDIM)
        state = start_ref[:, lanes]
        for c in range(rows // CHUNK):
            at = slice(c * CHUNK, (c + 1) * CHUNK)
            heard = heard_ref[at, lanes] + dot_wide(decayed_ref[at, lanes], state, NT)
            spread = lax.rsqrt(jnp.mean(heard * heard, axis=-1, keepdims=True) + EPSILON)
            mixed_ref[at, cols + h * RDIM : cols + (h + 1) * RDIM] = (
                heard * spread * gain_ref[...]
            ).astype(BF)
            total = cum_ref[(c + 1) * CHUNK - 1 : (c + 1) * CHUNK, lanes]
            state = state * jnp.exp(total) + growth_ref[c, :, lanes]

    finished(copies)
    far = whole_ref.shape[0]
    step = part_ref.shape[1] // far
    for f in range(far):
        weight = whole_ref[f].reshape(step, 2 * cols)
        part_ref[:, f * step : (f + 1) * step] = dot(mixed_ref[...], weight, NT).astype(BF)


VMEM = pl.BlockSpec(memory_space=pltpu.VMEM)
SMEM = pl.BlockSpec(memory_space=pltpu.SMEM)
HBM = pl.BlockSpec(memory_space=pltpu.HBM)


def call(kernel, outs, scratch, flops, moved, *args):
    return pl.pallas_call(
        kernel,
        out_shape=outs,
        in_specs=[SMEM if a.dtype == jnp.int32 else HBM if a.ndim == 5 else VMEM for a in args],
        out_specs=jax.tree.map(lambda _: VMEM, outs),
        scratch_shapes=scratch,
        cost_estimate=pl.CostEstimate(flops=flops, bytes_accessed=moved, transcendentals=0),
    )(*args)


def shape(dims, dtype):
    return jax.ShapeDtypeStruct(dims, dtype)


def side_by_side(*arrays):
    width = sum(a.shape[1] for a in arrays)
    total, at = None, 0
    for a in arrays:
        padded = jnp.pad(a, ((0, 0), (at, width - at - a.shape[1])))
        total = padded if total is None else total + padded
        at += a.shape[1]
    return total


def over_cores(x):
    return lax.ppermute(x, CORE, [(0, 1), (1, 0)])


def layer(
    tokens,
    norm_gain,
    pool_in_weight,
    query_weight,
    forget_weight,
    input_weight,
    forget_gap,
    decay_shift,
    out_gain,
    pool_out_weight,
    recur_out_weight,
):
    width = tokens.shape[1]
    cols = query_weight.shape[1]
    tp = lax.axis_size("tp")
    rows = tokens.shape[0] * tp
    devices = lax.axis_size(SP)
    info = jnp.stack(
        [
            lax.axis_index(CORE),
            lax.axis_index("tp"),
            lax.axis_index(SP) * rows,
            lax.axis_index(ACROSS),
            lax.axis_index(DEPTH),
        ]
    ).astype(jnp.int32)

    pieces = ring_gather(tokens, "tp")
    weights = side_by_side(
        forget_weight,
        input_weight,
        query_weight,
        pool_in_weight,
        pool_out_weight.T,
        recur_out_weight.T,
    )
    weights = sent_to_all(weights, FAR)
    weights = sent_to_all(weights, NEAR)
    inner = sent_to_all(weights[..., : 4 * cols], ACROSS)
    inner_other = over_cores(inner)
    outer = sent_to_all(weights[..., 4 * cols :], ACROSS)
    outer_other = over_cores(outer)
    blocks = outer.shape[2], outer.shape[1], outer.shape[0], 2, outer.shape[3], 2 * cols
    whole = [
        pltpu.VMEM(blocks, BF),
        pltpu.SemaphoreType.DMA((2 * outer.shape[0] * outer.shape[1],)),
    ]

    normed, values, opened, cum, growth, payload = call(
        state_kernel,
        [
            shape((rows, width), BF),
            shape((rows, cols), BF),
            shape((rows, cols), F32),
            shape((rows, cols), F32),
            shape((rows // CHUNK, RDIM, cols), F32),
            shape((RDIM, 2 * cols), F32),
        ],
        [*whole, pltpu.VMEM((rows, 2 * cols), F32)],
        4 * rows * width * cols,
        8 << 20,
        info,
        *pieces,
        norm_gain[None, :],
        inner,
        inner_other,
        forget_gap[None, :],
        decay_shift.T,
    )

    plane = lax.axis_size(PLANE)
    slab = RDIM // plane
    got = lax.all_to_all(payload, PLANE, split_axis=0, concat_axis=0, tiled=True)
    before, faded, total = call(
        plane_kernel,
        [
            shape((plane, slab, cols), F32),
            shape((plane, cols), F32),
            shape((slab + 16, cols), BF),
        ],
        [],
        1 << 20,
        1 << 19,
        got.reshape(plane, slab, 2 * cols),
    )
    totals = sent_to_all(total, DEPTH)
    start = call(
        depth_kernel,
        shape((plane, slab, cols), F32),
        [],
        1 << 20,
        1 << 19,
        info,
        totals,
        before,
        faded,
    )
    start = lax.all_to_all(
        start.reshape(RDIM, cols), PLANE, split_axis=0, concat_axis=0, tiled=True
    )
    pooled, decayed, heard = call(
        inner_kernel,
        [shape((rows, cols), BF), shape((rows, cols), F32), shape((rows, cols), F32)],
        [*whole, pltpu.VMEM((rows, 2 * cols), F32)],
        4 * rows * width * cols,
        8 << 20,
        info,
        normed,
        inner,
        inner_other,
        values,
        opened,
        cum,
    )
    order = [(i - 1, i) for i in range(1, devices)]
    rim = lax.ppermute(pooled[rows - RIM :], SP, order)
    part = call(
        final_kernel,
        shape((rows, width), BF),
        [*whole, pltpu.VMEM((rows, 2 * cols), BF)],
        4 * rows * width * cols,
        8 << 20,
        info,
        start,
        growth,
        cum,
        decayed,
        heard,
        pooled,
        rim,
        out_gain[None, :],
        outer,
        outer_other,
    )
    parts = lax.all_to_all(
        part.reshape(tp, rows // tp, width), "tp", split_axis=0, concat_axis=0, tiled=True
    )
    return jnp.sum(parts.astype(F32), axis=0).astype(BF)


def solution(mesh):
    split = Mesh(mesh.devices.reshape(4, 4, 4, 2, mesh.shape["tp"]), SP_TP)
    in_specs = (
        P(SP_TP, None),
        P(),
        P(SP, "tp"),
        P(SP, "tp"),
        P(SP, "tp"),
        P(SP, "tp"),
        P("tp"),
        P("tp", SP),
        P(),
        P("tp", SP),
        P("tp", SP),
    )
    out_specs = P(SP_TP, None)
    return jax.shard_map(layer, mesh=split, in_specs=in_specs, out_specs=out_specs, check_vma=False)
```

```python
import jax
import jax.numpy as jnp
from jax import lax
from jax.experimental import pallas as pl
from jax.experimental.pallas import tpu as pltpu
from jax.sharding import Mesh
from jax.sharding import PartitionSpec as P


GROUPS = 4
RDIM = 128
CHUNK = 128
RIM = 16
FAR, NEAR, ACROSS, CORE = "sp_f", "sp_n", "sp_x", "sp_c"
DEPTH = (FAR, NEAR)
PLANE = (ACROSS, CORE)
SP = (FAR, NEAR, ACROSS, CORE)
SP_TP = (FAR, NEAR, ACROSS, CORE, "tp")
EPSILON = 1e-06
BF = jnp.bfloat16
F32 = jnp.float32
NT = (((1,), (1,)), ((), ()))
TN = (((0,), (0,)), ((), ()))
NN = (((1,), (0,)), ((), ()))


def dot(a, b, dims=NN):
    return lax.dot_general(a, b, dims, preferred_element_type=F32)


def halves(x):
    high = x.astype(BF)
    return high, (x - high.astype(F32)).astype(BF)


def dot_wide(a, b, dims=NN):
    ah, al = halves(a)
    bh, bl = halves(b)
    return dot(ah, bh, dims) + (dot(ah, bl, dims) + dot(al, bh, dims))


def dot_left(a, b, dims=NN):
    ah, al = halves(a)
    return dot(ah, b, dims) + dot(al, b, dims)


def sent_to_all(x, axis):
    copies = jnp.broadcast_to(x, (lax.axis_size(axis), *x.shape))
    return lax.all_to_all(copies, axis, split_axis=0, concat_axis=0, tiled=True)


def ring_gather(x, axis):
    n = lax.axis_size(axis)
    pieces = [x]
    for shift in (1, -1, -2):
        pieces.append(lax.ppermute(x, axis, [(i, (i + shift) % n) for i in range(n)]))
    return pieces


def places(index, n):
    return [index, lax.rem(index + n - 1, n), lax.rem(index + 1, n), lax.rem(index + 2, n)]


def fetches(core, across, near, mine_ref, other_ref, lanes, whole_ref, sems):
    copies = []
    for i, x in enumerate(across):
        for j, n in enumerate(near):
            for side, from_ref in enumerate((mine_ref, other_ref)):
                to = core if side == 0 else 1 - core
                copies.append(
                    pltpu.make_async_copy(
                        from_ref.at[i, j, :, :, lanes],
                        whole_ref.at[:, n, x, to],
                        sems.at[len(copies)],
                    )
                )
    return copies


def started(copies):
    for copy in copies:
        copy.start()


def finished(copies):
    for copy in copies:
        copy.wait()


def state_kernel(
    info_ref,
    own_ref,
    before_ref,
    after_ref,
    far_ref,
    gain_ref,
    mine_ref,
    other_ref,
    gap_ref,
    shift_ref,
    normed_ref,
    values_ref,
    opened_ref,
    cum_ref,
    growth_ref,
    payload_ref,
    whole_ref,
    sems,
    both_ref,
):
    rows, _ = normed_ref.shape
    cols = gap_ref.shape[1]
    copies = fetches(
        info_ref[0],
        range(mine_ref.shape[0]),
        range(mine_ref.shape[1]),
        mine_ref,
        other_ref,
        slice(None),
        whole_ref,
        sems,
    )
    started(copies)
    block = own_ref.shape[0]
    own, before, after, far = places(info_ref[1], rows // block)

    def norm(from_ref, start, i):
        floats = from_ref[pl.ds(pl.multiple_of(i * 32, 32), 32), :].astype(F32)
        scale = lax.rsqrt(jnp.mean(floats * floats, axis=-1, keepdims=True) + EPSILON)
        at = pl.ds(pl.multiple_of(start + i * 32, 32), 32)
        normed_ref[at, :] = (floats * scale * gain_ref[...]).astype(BF)

    def norm_all(i, carry):
        norm(own_ref, own * block, i)
        norm(before_ref, before * block, i)
        norm(after_ref, after * block, i)
        norm(far_ref, far * block, i)
        return carry

    lax.fori_loop(0, block // 32, norm_all, 0)
    finished(copies)
    both_ref[...] = dot(normed_ref[...], whole_ref[...].reshape(-1, 2 * cols))
    row = lax.broadcasted_iota(jnp.int32, (CHUNK, CHUNK), 0)
    col = lax.broadcasted_iota(jnp.int32, (CHUNK, CHUNK), 1)
    tril = (row >= col).astype(BF)
    heads = cols // RDIM
    for h in range(heads):
        lanes = slice(h * RDIM, (h + 1) * RDIM)
        state = jnp.zeros((RDIM, RDIM), F32)
        faded = jnp.zeros((1, RDIM), F32)
        for c in range(rows // CHUNK):
            at = slice(c * CHUNK, (c + 1) * CHUNK)
            pre = both_ref[at, lanes].astype(BF).astype(F32)
            values = both_ref[at, cols + h * RDIM : cols + (h + 1) * RDIM].astype(BF)
            opened = gap_ref[:, lanes] / (1.0 + jnp.exp(pre))
            decay = jnp.log1p(-opened) + shift_ref[at, h : h + 1]
            d0, d1 = halves(decay)
            d2 = (decay - d0.astype(F32) - d1.astype(F32)).astype(BF)
            cum = dot(tril, d0) + (dot(tril, d1) + dot(tril, d2))
            total = cum[CHUNK - 1 :, :]
            growth = dot_left_t(values, opened * jnp.exp(total - cum))
            values_ref[at, lanes] = values
            opened_ref[at, lanes] = opened
            cum_ref[at, lanes] = cum
            growth_ref[c, :, lanes] = growth
            state = state * jnp.exp(total) + growth
            faded = faded + total
        payload_ref[:, lanes] = state
        payload_ref[:, cols + h * RDIM : cols + (h + 1) * RDIM] = jnp.broadcast_to(faded, (RDIM, RDIM))


def dot_left_t(values, key):
    kh, kl = halves(key)
    return dot(values, kh, TN) + dot(values, kl, TN)


def plane_kernel(got_ref, before_ref, faded_ref, total_ref):
    rows = got_ref.shape[1]
    cols = before_ref.shape[2]
    state = jnp.zeros((rows, cols), F32)
    faded = jnp.zeros((1, cols), F32)
    for d in range(got_ref.shape[0]):
        fade = got_ref[d, :1, cols:]
        before_ref[d] = state
        faded_ref[d : d + 1, :] = faded
        state = state * jnp.exp(fade) + got_ref[d, :, :cols]
        faded = faded + fade
    high = faded.astype(BF).astype(F32)
    row = lax.broadcasted_iota(jnp.int32, (8, cols), 0)
    fades = jnp.where(row == 0, high, jnp.where(row == 1, faded - high, 0.0))
    total = jnp.concatenate([state, fades], axis=0).astype(BF)
    for z in range(total_ref.shape[0]):
        total_ref[z] = total


def depth_kernel(info_ref, totals_ref, before_ref, faded_ref, start_ref):
    planes = totals_ref.shape[0]
    devices, rows, cols = before_ref.shape
    state = jnp.zeros((rows, cols), F32)
    for z in range(planes):
        got = totals_ref[z].astype(F32)
        fade = got[rows : rows + 1] + got[rows + 1 : rows + 2]
        state = jnp.where(z < info_ref[4], state * jnp.exp(fade) + got[:rows], state)
    for d in range(devices):
        start_ref[d] = before_ref[d] + jnp.exp(faded_ref[d : d + 1, :]) * state


def inner_kernel(
    info_ref,
    normed_ref,
    mine_ref,
    other_ref,
    values_ref,
    opened_ref,
    cum_ref,
    pooled_ref,
    decayed_ref,
    heard_ref,
    whole_ref,
    sems,
    both_ref,
):
    rows, cols = values_ref.shape
    copies = fetches(
        info_ref[0],
        places(info_ref[3], mine_ref.shape[0]),
        places(info_ref[5], mine_ref.shape[1]),
        mine_ref,
        other_ref,
        slice(0, 2 * cols),
        whole_ref,
        sems,
    )
    started(copies)
    finished(copies)
    both_ref[...] = dot(normed_ref[...], whole_ref[...].reshape(-1, 2 * cols))
    pooled_ref[...] = both_ref[:, cols:].astype(BF)
    row = lax.broadcasted_iota(jnp.int32, (CHUNK, CHUNK), 0)
    col = lax.broadcasted_iota(jnp.int32, (CHUNK, CHUNK), 1)
    for h in range(cols // RDIM):
        lanes = slice(h * RDIM, (h + 1) * RDIM)
        for c in range(rows // CHUNK):
            at = slice(c * CHUNK, (c + 1) * CHUNK)
            cum = cum_ref[at, lanes]
            query = both_ref[at, lanes].astype(BF).astype(F32) * jnp.exp(cum)
            key = opened_ref[at, lanes] * jnp.exp(-cum)
            scores = jnp.where(row >= col, dot_wide(query, key, NT), 0.0)
            decayed_ref[at, lanes] = query
            heard_ref[at, lanes] = dot_left(scores, values_ref[at, lanes])


def final_kernel(
    info_ref,
    start_ref,
    growth_ref,
    cum_ref,
    decayed_ref,
    heard_ref,
    pooled_ref,
    rim_ref,
    gain_ref,
    mine_ref,
    other_ref,
    part_ref,
    whole_ref,
    sems,
    mixed_ref,
):
    rows, cols = cum_ref.shape
    copies = fetches(
        info_ref[0],
        places(info_ref[3], mine_ref.shape[0]),
        places(info_ref[5], mine_ref.shape[1]),
        mine_ref,
        other_ref,
        slice(2 * cols, 4 * cols),
        whole_ref,
        sems,
    )
    started(copies)
    group = info_ref[1]
    padded = jnp.concatenate([rim_ref[...], pooled_ref[...]], axis=0).astype(F32)
    running = padded
    chosen = None
    for level in range(GROUPS):
        running = running + pltpu.roll(running, 2**level, 0)
        chosen = running if chosen is None else jnp.where(group == level, running, chosen)
    width = jnp.left_shift(jnp.int32(2), group)
    position = info_ref[2] + lax.broadcasted_iota(jnp.int32, (rows, cols), 0)
    divisor = jnp.minimum(position + 1, width).astype(F32)
    mixed_ref[:, :cols] = (chosen[RIM:] / divisor - padded[RIM:]).astype(BF)
    for h in range(cols // RDIM):
        lanes = slice(h * RDIM, (h + 1) * RDIM)
        state = start_ref[:, lanes]
        for c in range(rows // CHUNK):
            at = slice(c * CHUNK, (c + 1) * CHUNK)
            heard = heard_ref[at, lanes] + dot_wide(decayed_ref[at, lanes], state, NT)
            spread = lax.rsqrt(jnp.mean(heard * heard, axis=-1, keepdims=True) + EPSILON)
            mixed_ref[at, cols + h * RDIM : cols + (h + 1) * RDIM] = (
                heard * spread * gain_ref[...]
            ).astype(BF)
            total = cum_ref[(c + 1) * CHUNK - 1 : (c + 1) * CHUNK, lanes]
            state = state * jnp.exp(total) + growth_ref[c, :, lanes]

    finished(copies)
    far = whole_ref.shape[0]
    step = part_ref.shape[1] // far
    for f in range(far):
        weight = whole_ref[f].reshape(step, 2 * cols)
        part_ref[:, f * step : (f + 1) * step] = dot(mixed_ref[...], weight, NT).astype(BF)


VMEM = pl.BlockSpec(memory_space=pltpu.VMEM)
SMEM = pl.BlockSpec(memory_space=pltpu.SMEM)
HBM = pl.BlockSpec(memory_space=pltpu.HBM)


def call(kernel, outs, scratch, flops, moved, *args):
    return pl.pallas_call(
        kernel,
        out_shape=outs,
        in_specs=[SMEM if a.dtype == jnp.int32 else HBM if a.ndim == 5 else VMEM for a in args],
        out_specs=jax.tree.map(lambda _: VMEM, outs),
        scratch_shapes=scratch,
        cost_estimate=pl.CostEstimate(flops=flops, bytes_accessed=moved, transcendentals=0),
    )(*args)


def shape(dims, dtype):
    return jax.ShapeDtypeStruct(dims, dtype)


def side_by_side(*arrays):
    width = sum(a.shape[1] for a in arrays)
    total, at = None, 0
    for a in arrays:
        padded = jnp.pad(a, ((0, 0), (at, width - at - a.shape[1])))
        total = padded if total is None else total + padded
        at += a.shape[1]
    return total


def over_cores(x):
    return lax.ppermute(x, CORE, [(0, 1), (1, 0)])


def layer(
    tokens,
    norm_gain,
    pool_in_weight,
    query_weight,
    forget_weight,
    input_weight,
    forget_gap,
    decay_shift,
    out_gain,
    pool_out_weight,
    recur_out_weight,
):
    width = tokens.shape[1]
    cols = query_weight.shape[1]
    tp = lax.axis_size("tp")
    rows = tokens.shape[0] * tp
    devices = lax.axis_size(SP)
    info = jnp.stack(
        [
            lax.axis_index(CORE),
            lax.axis_index("tp"),
            lax.axis_index(SP) * rows,
            lax.axis_index(ACROSS),
            lax.axis_index(DEPTH),
            lax.axis_index(NEAR),
        ]
    ).astype(jnp.int32)

    pieces = ring_gather(tokens, "tp")
    weights = side_by_side(
        forget_weight,
        input_weight,
        query_weight,
        pool_in_weight,
        pool_out_weight.T,
        recur_out_weight.T,
    )
    weights = sent_to_all(weights, FAR)
    first = sent_to_all(weights[..., : 2 * cols], NEAR)
    first = sent_to_all(first, ACROSS)
    first_other = over_cores(first)
    rest = jnp.stack(ring_gather(weights[..., 2 * cols :], DEPTH))
    rest = jnp.stack(ring_gather(rest, ACROSS))
    rest_other = over_cores(rest)
    blocks = first.shape[2], first.shape[1], first.shape[0], 2, first.shape[3], 2 * cols
    whole = [
        pltpu.VMEM(blocks, BF),
        pltpu.SemaphoreType.DMA((2 * first.shape[0] * first.shape[1],)),
    ]

    normed, values, opened, cum, growth, payload = call(
        state_kernel,
        [
            shape((rows, width), BF),
            shape((rows, cols), BF),
            shape((rows, cols), F32),
            shape((rows, cols), F32),
            shape((rows // CHUNK, RDIM, cols), F32),
            shape((RDIM, 2 * cols), F32),
        ],
        [*whole, pltpu.VMEM((rows, 2 * cols), F32)],
        4 * rows * width * cols,
        8 << 20,
        info,
        *pieces,
        norm_gain[None, :],
        first,
        first_other,
        forget_gap[None, :],
        decay_shift.T,
    )

    plane = lax.axis_size(PLANE)
    slab = RDIM // plane
    got = lax.all_to_all(payload, PLANE, split_axis=0, concat_axis=0, tiled=True)
    before, faded, total = call(
        plane_kernel,
        [
            shape((plane, slab, cols), F32),
            shape((plane, cols), F32),
            shape((lax.axis_size(DEPTH), slab + 8, cols), BF),
        ],
        [],
        1 << 20,
        1 << 19,
        got.reshape(plane, slab, 2 * cols),
    )
    totals = lax.all_to_all(total, DEPTH, split_axis=0, concat_axis=0, tiled=True)
    start = call(
        depth_kernel,
        shape((plane, slab, cols), F32),
        [],
        1 << 20,
        1 << 19,
        info,
        totals,
        before,
        faded,
    )
    start = lax.all_to_all(
        start.reshape(RDIM, cols), PLANE, split_axis=0, concat_axis=0, tiled=True
    )
    pooled, decayed, heard = call(
        inner_kernel,
        [shape((rows, cols), BF), shape((rows, cols), F32), shape((rows, cols), F32)],
        [*whole, pltpu.VMEM((rows, 2 * cols), F32)],
        4 * rows * width * cols,
        8 << 20,
        info,
        normed,
        rest,
        rest_other,
        values,
        opened,
        cum,
    )
    order = [(i - 1, i) for i in range(1, devices)]
    rim = lax.ppermute(pooled[rows - RIM :], SP, order)
    part = call(
        final_kernel,
        shape((rows, width), BF),
        [*whole, pltpu.VMEM((rows, 2 * cols), BF)],
        4 * rows * width * cols,
        8 << 20,
        info,
        start,
        growth,
        cum,
        decayed,
        heard,
        pooled,
        rim,
        out_gain[None, :],
        rest,
        rest_other,
    )
    parts = lax.all_to_all(
        part.reshape(tp, rows // tp, width), "tp", split_axis=0, concat_axis=0, tiled=True
    )
    return jnp.sum(parts.astype(F32), axis=0).astype(BF)


def solution(mesh):
    split = Mesh(mesh.devices.reshape(4, 4, 4, 2, mesh.shape["tp"]), SP_TP)
    in_specs = (
        P(SP_TP, None),
        P(),
        P(SP, "tp"),
        P(SP, "tp"),
        P(SP, "tp"),
        P(SP, "tp"),
        P("tp"),
        P("tp", SP),
        P(),
        P("tp", SP),
        P("tp", SP),
    )
    out_specs = P(SP_TP, None)
    return jax.shard_map(layer, mesh=split, in_specs=in_specs, out_specs=out_specs, check_vma=False)
```

```python
import jax
import jax.numpy as jnp
from jax import lax
from jax.experimental import pallas as pl
from jax.experimental.pallas import tpu as pltpu
from jax.sharding import Mesh
from jax.sharding import PartitionSpec as P


GROUPS = 4
RDIM = 128
CHUNK = 128
RIM = 16
FAR, NEAR, ACROSS, CORE = "sp_f", "sp_n", "sp_x", "sp_c"
DEPTH = (FAR, NEAR)
PLANE = (ACROSS, CORE)
SP = (FAR, NEAR, ACROSS, CORE)
SP_TP = (FAR, NEAR, ACROSS, CORE, "tp")
EPSILON = 1e-06
BF = jnp.bfloat16
F32 = jnp.float32
NT = (((1,), (1,)), ((), ()))
TN = (((0,), (0,)), ((), ()))
NN = (((1,), (0,)), ((), ()))


def dot(a, b, dims=NN):
    return lax.dot_general(a, b, dims, preferred_element_type=F32)


def halves(x):
    high = x.astype(BF)
    return high, (x - high.astype(F32)).astype(BF)


def dot_wide(a, b, dims=NN):
    ah, al = halves(a)
    bh, bl = halves(b)
    return dot(ah, bh, dims) + (dot(ah, bl, dims) + dot(al, bh, dims))


def dot_left(a, b, dims=NN):
    ah, al = halves(a)
    return dot(ah, b, dims) + dot(al, b, dims)


def sent_to_all(x, axis):
    copies = jnp.broadcast_to(x, (lax.axis_size(axis), *x.shape))
    return lax.all_to_all(copies, axis, split_axis=0, concat_axis=0, tiled=True)


def ring_gather(x, axis):
    n = lax.axis_size(axis)
    pieces = [x]
    for shift in (1, -1, -2):
        pieces.append(lax.ppermute(x, axis, [(i, (i + shift) % n) for i in range(n)]))
    return pieces


def places(index, n):
    return [index, lax.rem(index + n - 1, n), lax.rem(index + 1, n), lax.rem(index + 2, n)]


def fetches(core, across, near, mine_ref, other_ref, lanes, whole_ref, sems):
    copies = []
    for i, x in enumerate(across):
        for j, n in enumerate(near):
            for side, from_ref in enumerate((mine_ref, other_ref)):
                to = core if side == 0 else 1 - core
                copies.append(
                    pltpu.make_async_copy(
                        from_ref.at[i, j, :, :, lanes],
                        whole_ref.at[:, n, x, to],
                        sems.at[len(copies)],
                    )
                )
    return copies


def started(copies):
    for copy in copies:
        copy.start()


def finished(copies):
    for copy in copies:
        copy.wait()


def fade_rows(faded):
    high = faded.astype(BF).astype(F32)
    row = lax.broadcasted_iota(jnp.int32, (8, faded.shape[1]), 0)
    return jnp.where(row == 0, high, jnp.where(row == 1, faded - high, 0.0))


def fade_of(block):
    rows = block.shape[0]
    return block[rows - 8 : rows - 7] + block[rows - 7 : rows - 6]


def state_kernel(
    info_ref,
    own_ref,
    before_ref,
    after_ref,
    far_ref,
    gain_ref,
    mine_ref,
    other_ref,
    gap_ref,
    shift_ref,
    normed_out_ref,
    values_ref,
    opened_ref,
    cum_ref,
    growth_ref,
    payload_ref,
    whole_ref,
    sems,
    both_ref,
    tokens_ref,
    normed_ref,
    token_sems,
):
    rows, _ = normed_ref.shape
    cols = gap_ref.shape[1]
    block = own_ref.shape[0]
    spots = places(info_ref[1], rows // block)
    token_copies = [
        pltpu.make_async_copy(from_ref, tokens_ref.at[k], token_sems.at[k])
        for k, from_ref in enumerate((own_ref, before_ref, after_ref, far_ref))
    ]
    started(token_copies)
    copies = fetches(
        info_ref[0],
        range(mine_ref.shape[0]),
        range(mine_ref.shape[1]),
        mine_ref,
        other_ref,
        slice(None),
        whole_ref,
        sems,
    )
    started(copies)
    for k, spot in enumerate(spots):
        token_copies[k].wait()

        def norm(i, carry):
            floats = tokens_ref[k, pl.ds(pl.multiple_of(i * 32, 32), 32), :].astype(F32)
            scale = lax.rsqrt(jnp.mean(floats * floats, axis=-1, keepdims=True) + EPSILON)
            at = pl.ds(pl.multiple_of(spot * block + i * 32, 32), 32)
            normed_ref[at, :] = (floats * scale * gain_ref[...]).astype(BF)
            return carry

        lax.fori_loop(0, block // 32, norm, 0)
    handing = pltpu.make_async_copy(normed_ref, normed_out_ref, token_sems.at[len(spots)])
    handing.start()
    finished(copies)
    both_ref[...] = dot(normed_ref[...], whole_ref[...].reshape(-1, 2 * cols))
    row = lax.broadcasted_iota(jnp.int32, (CHUNK, CHUNK), 0)
    col = lax.broadcasted_iota(jnp.int32, (CHUNK, CHUNK), 1)
    tril = (row >= col).astype(BF)
    plane, height, _ = payload_ref.shape
    slab = height - 8
    for h in range(cols // RDIM):
        lanes = slice(h * RDIM, (h + 1) * RDIM)
        state = jnp.zeros((RDIM, RDIM), F32)
        faded = jnp.zeros((1, RDIM), F32)
        for c in range(rows // CHUNK):
            at = slice(c * CHUNK, (c + 1) * CHUNK)
            pre = both_ref[at, lanes].astype(BF).astype(F32)
            values = both_ref[at, cols + h * RDIM : cols + (h + 1) * RDIM].astype(BF)
            opened = gap_ref[:, lanes] / (1.0 + jnp.exp(pre))
            shift = jnp.broadcast_to(shift_ref[h : h + 1, at], (RDIM, CHUNK)).T
            decay = jnp.log1p(-opened) + shift
            d0, d1 = halves(decay)
            d2 = (decay - d0.astype(F32) - d1.astype(F32)).astype(BF)
            cum = dot(tril, d0) + (dot(tril, d1) + dot(tril, d2))
            total = cum[CHUNK - 1 :, :]
            growth = dot_left_t(values, opened * jnp.exp(total - cum))
            values_ref[at, lanes] = values
            opened_ref[at, lanes] = opened
            cum_ref[at, lanes] = cum
            growth_ref[c, :, lanes] = growth
            state = state * jnp.exp(total) + growth
            faded = faded + total
        fades = fade_rows(faded)
        for d in range(plane):
            block_d = jnp.concatenate([state[d * slab : (d + 1) * slab], fades], axis=0)
            payload_ref[d, :, lanes] = block_d.astype(BF)
    handing.wait()


def dot_left_t(values, key):
    kh, kl = halves(key)
    return dot(values, kh, TN) + dot(values, kl, TN)


def plane_kernel(got_ref, before_ref, faded_ref, total_ref):
    _, rows, cols = before_ref.shape
    state = jnp.zeros((rows, cols), F32)
    faded = jnp.zeros((1, cols), F32)
    for d in range(got_ref.shape[0]):
        got = got_ref[d].astype(F32)
        fade = fade_of(got)
        before_ref[d] = state
        faded_ref[d : d + 1, :] = faded
        state = state * jnp.exp(fade) + got[:rows]
        faded = faded + fade
    total = jnp.concatenate([state, fade_rows(faded)], axis=0).astype(BF)
    for z in range(total_ref.shape[0]):
        total_ref[z] = total


def depth_kernel(info_ref, totals_ref, before_ref, faded_ref, start_ref):
    planes = totals_ref.shape[0]
    devices, rows, cols = before_ref.shape
    state = jnp.zeros((rows, cols), F32)
    for z in range(planes):
        got = totals_ref[z].astype(F32)
        new = state * jnp.exp(fade_of(got)) + got[:rows]
        state = jnp.where(z < info_ref[4], new, state)
    for d in range(devices):
        start_ref[d] = (before_ref[d] + jnp.exp(faded_ref[d : d + 1, :]) * state).astype(BF)


def inner_kernel(
    info_ref,
    normed_ref,
    mine_ref,
    other_ref,
    values_ref,
    opened_ref,
    cum_ref,
    pooled_ref,
    decayed_ref,
    heard_ref,
    whole_ref,
    sems,
    both_ref,
    held_ref,
    held_sem,
):
    rows, cols = values_ref.shape
    bringing = pltpu.make_async_copy(normed_ref, held_ref, held_sem.at[0])
    bringing.start()
    copies = fetches(
        info_ref[0],
        places(info_ref[3], mine_ref.shape[0]),
        places(info_ref[5], mine_ref.shape[1]),
        mine_ref,
        other_ref,
        slice(0, 2 * cols),
        whole_ref,
        sems,
    )
    started(copies)
    finished(copies)
    bringing.wait()
    both_ref[...] = dot(held_ref[...], whole_ref[...].reshape(-1, 2 * cols))
    pooled_ref[...] = both_ref[:, cols:].astype(BF)
    row = lax.broadcasted_iota(jnp.int32, (CHUNK, CHUNK), 0)
    col = lax.broadcasted_iota(jnp.int32, (CHUNK, CHUNK), 1)
    for h in range(cols // RDIM):
        lanes = slice(h * RDIM, (h + 1) * RDIM)
        for c in range(rows // CHUNK):
            at = slice(c * CHUNK, (c + 1) * CHUNK)
            cum = cum_ref[at, lanes]
            query = both_ref[at, lanes].astype(BF).astype(F32) * jnp.exp(cum)
            key = opened_ref[at, lanes] * jnp.exp(-cum)
            scores = jnp.where(row >= col, dot_wide(query, key, NT), 0.0)
            decayed_ref[at, lanes] = query
            heard_ref[at, lanes] = dot_left(scores, values_ref[at, lanes])


def final_kernel(
    info_ref,
    start_ref,
    growth_ref,
    cum_ref,
    decayed_ref,
    heard_ref,
    pooled_ref,
    rim_ref,
    gain_ref,
    mine_ref,
    other_ref,
    part_ref,
    whole_ref,
    sems,
    mixed_ref,
):
    rows, cols = cum_ref.shape
    copies = fetches(
        info_ref[0],
        places(info_ref[3], mine_ref.shape[0]),
        places(info_ref[5], mine_ref.shape[1]),
        mine_ref,
        other_ref,
        slice(2 * cols, 4 * cols),
        whole_ref,
        sems,
    )
    started(copies)
    group = info_ref[1]
    padded = jnp.concatenate([rim_ref[...], pooled_ref[...]], axis=0).astype(F32)
    running = padded
    chosen = None
    for level in range(GROUPS):
        running = running + pltpu.roll(running, 2**level, 0)
        chosen = running if chosen is None else jnp.where(group == level, running, chosen)
    width = jnp.left_shift(jnp.int32(2), group)
    position = info_ref[2] + lax.broadcasted_iota(jnp.int32, (rows, cols), 0)
    divisor = jnp.minimum(position + 1, width).astype(F32)
    mixed_ref[:, :cols] = (chosen[RIM:] / divisor - padded[RIM:]).astype(BF)
    for h in range(cols // RDIM):
        lanes = slice(h * RDIM, (h + 1) * RDIM)
        state = start_ref[:, lanes].astype(F32)
        for c in range(rows // CHUNK):
            at = slice(c * CHUNK, (c + 1) * CHUNK)
            heard = heard_ref[at, lanes] + dot_wide(decayed_ref[at, lanes], state, NT)
            spread = lax.rsqrt(jnp.mean(heard * heard, axis=-1, keepdims=True) + EPSILON)
            mixed_ref[at, cols + h * RDIM : cols + (h + 1) * RDIM] = (
                heard * spread * gain_ref[...]
            ).astype(BF)
            total = cum_ref[(c + 1) * CHUNK - 1 : (c + 1) * CHUNK, lanes]
            state = state * jnp.exp(total) + growth_ref[c, :, lanes]

    finished(copies)
    far = whole_ref.shape[0]
    step = part_ref.shape[1] // far
    for f in range(far):
        weight = whole_ref[f].reshape(step, 2 * cols)
        part_ref[:, f * step : (f + 1) * step] = dot(mixed_ref[...], weight, NT).astype(BF)


VMEM = pl.BlockSpec(memory_space=pltpu.VMEM)
SMEM = pl.BlockSpec(memory_space=pltpu.SMEM)
HBM = pl.BlockSpec(memory_space=pltpu.HBM)


def spec_of(a):
    if a.dtype == jnp.int32:
        return SMEM
    return HBM if a.size * a.dtype.itemsize >= 1 << 19 and a.dtype == BF else VMEM


def call(kernel, outs, scratch, flops, moved, *args, out_specs=None):
    return pl.pallas_call(
        kernel,
        out_shape=outs,
        in_specs=[spec_of(a) for a in args],
        out_specs=out_specs or jax.tree.map(lambda _: VMEM, outs),
        scratch_shapes=scratch,
        cost_estimate=pl.CostEstimate(flops=flops, bytes_accessed=moved, transcendentals=0),
    )(*args)


def shape(dims, dtype):
    return jax.ShapeDtypeStruct(dims, dtype)


def side_by_side(*arrays):
    width = sum(a.shape[1] for a in arrays)
    total, at = None, 0
    for a in arrays:
        padded = jnp.pad(a, ((0, 0), (at, width - at - a.shape[1])))
        total = padded if total is None else total + padded
        at += a.shape[1]
    return total


def over_cores(x):
    return lax.ppermute(x, CORE, [(0, 1), (1, 0)])


def layer(
    tokens,
    norm_gain,
    pool_in_weight,
    query_weight,
    forget_weight,
    input_weight,
    forget_gap,
    decay_shift,
    out_gain,
    pool_out_weight,
    recur_out_weight,
):
    width = tokens.shape[1]
    cols = query_weight.shape[1]
    tp = lax.axis_size("tp")
    rows = tokens.shape[0] * tp
    devices = lax.axis_size(SP)
    info = jnp.stack(
        [
            lax.axis_index(CORE),
            lax.axis_index("tp"),
            lax.axis_index(SP) * rows,
            lax.axis_index(ACROSS),
            lax.axis_index(DEPTH),
            lax.axis_index(NEAR),
        ]
    ).astype(jnp.int32)

    pieces = ring_gather(tokens, "tp")
    weights = side_by_side(
        forget_weight,
        input_weight,
        query_weight,
        pool_in_weight,
        pool_out_weight.T,
        recur_out_weight.T,
    )
    weights = sent_to_all(weights, FAR)
    first = sent_to_all(weights[..., : 2 * cols], NEAR)
    first = sent_to_all(first, ACROSS)
    first_other = over_cores(first)
    rest = jnp.stack(ring_gather(weights[..., 2 * cols :], DEPTH))
    rest = jnp.stack(ring_gather(rest, ACROSS))
    rest_other = over_cores(rest)
    blocks = first.shape[2], first.shape[1], first.shape[0], 2, first.shape[3], 2 * cols
    whole = [
        pltpu.VMEM(blocks, BF),
        pltpu.SemaphoreType.DMA((2 * first.shape[0] * first.shape[1],)),
    ]

    plane = lax.axis_size(PLANE)
    slab = RDIM // plane
    normed, values, opened, cum, growth, payload = call(
        state_kernel,
        [
            shape((rows, width), BF),
            shape((rows, cols), BF),
            shape((rows, cols), F32),
            shape((rows, cols), F32),
            shape((rows // CHUNK, RDIM, cols), F32),
            shape((plane, slab + 8, cols), BF),
        ],
        [
            *whole,
            pltpu.VMEM((rows, 2 * cols), F32),
            pltpu.VMEM((tp, rows // tp, width), BF),
            pltpu.VMEM((rows, width), BF),
            pltpu.SemaphoreType.DMA((tp + 1,)),
        ],
        4 * rows * width * cols,
        8 << 20,
        info,
        *pieces,
        norm_gain[None, :],
        first,
        first_other,
        forget_gap[None, :],
        decay_shift,
        out_specs=[HBM, VMEM, VMEM, VMEM, VMEM, VMEM],
    )
    got = lax.all_to_all(payload, PLANE, split_axis=0, concat_axis=0, tiled=True)
    before, faded, total = call(
        plane_kernel,
        [
            shape((plane, slab, cols), F32),
            shape((plane, cols), F32),
            shape((lax.axis_size(DEPTH), slab + 8, cols), BF),
        ],
        [],
        1 << 20,
        1 << 19,
        got,
    )
    totals = lax.all_to_all(total, DEPTH, split_axis=0, concat_axis=0, tiled=True)
    start = call(
        depth_kernel,
        shape((plane, slab, cols), BF),
        [],
        1 << 20,
        1 << 19,
        info,
        totals,
        before,
        faded,
    )
    start = lax.all_to_all(
        start.reshape(RDIM, cols), PLANE, split_axis=0, concat_axis=0, tiled=True
    )
    pooled, decayed, heard = call(
        inner_kernel,
        [shape((rows, cols), BF), shape((rows, cols), F32), shape((rows, cols), F32)],
        [
            *whole,
            pltpu.VMEM((rows, 2 * cols), F32),
            pltpu.VMEM((rows, width), BF),
            pltpu.SemaphoreType.DMA((1,)),
        ],
        4 * rows * width * cols,
        8 << 20,
        info,
        normed,
        rest,
        rest_other,
        values,
        opened,
        cum,
    )
    order = [(i - 1, i) for i in range(1, devices)]
    rim = lax.ppermute(pooled[rows - RIM :], SP, order)
    part = call(
        final_kernel,
        shape((rows, width), BF),
        [*whole, pltpu.VMEM((rows, 2 * cols), BF)],
        4 * rows * width * cols,
        8 << 20,
        info,
        start,
        growth,
        cum,
        decayed,
        heard,
        pooled,
        rim,
        out_gain[None, :],
        rest,
        rest_other,
    )
    parts = lax.all_to_all(
        part.reshape(tp, rows // tp, width), "tp", split_axis=0, concat_axis=0, tiled=True
    )
    return jnp.sum(parts.astype(F32), axis=0).astype(BF)


def solution(mesh):
    split = Mesh(mesh.devices.reshape(4, 4, 4, 2, mesh.shape["tp"]), SP_TP)
    in_specs = (
        P(SP_TP, None),
        P(),
        P(SP, "tp"),
        P(SP, "tp"),
        P(SP, "tp"),
        P(SP, "tp"),
        P("tp"),
        P("tp", SP),
        P(),
        P("tp", SP),
        P("tp", SP),
    )
    out_specs = P(SP_TP, None)
    return jax.shard_map(layer, mesh=split, in_specs=in_specs, out_specs=out_specs, check_vma=False)
```

```python
import jax
import jax.numpy as jnp
from jax import lax
from jax.experimental import pallas as pl
from jax.experimental.pallas import tpu as pltpu
from jax.sharding import Mesh
from jax.sharding import PartitionSpec as P


GROUPS = 4
RDIM = 128
CHUNK = 128
RIM = 16
FAR, NEAR, ACROSS, CORE = "sp_f", "sp_n", "sp_x", "sp_c"
DEPTH = (FAR, NEAR)
PLANE = (ACROSS, CORE)
SP = (FAR, NEAR, ACROSS, CORE)
SP_TP = (FAR, NEAR, ACROSS, CORE, "tp")
EPSILON = 1e-06
BF = jnp.bfloat16
F32 = jnp.float32
NT = (((1,), (1,)), ((), ()))
TN = (((0,), (0,)), ((), ()))
NN = (((1,), (0,)), ((), ()))


def dot(a, b, dims=NN):
    return lax.dot_general(a, b, dims, preferred_element_type=F32)


def halves(x):
    high = x.astype(BF)
    return high, (x - high.astype(F32)).astype(BF)


def dot_wide(a, b, dims=NN):
    ah, al = halves(a)
    bh, bl = halves(b)
    return dot(ah, bh, dims) + (dot(ah, bl, dims) + dot(al, bh, dims))


def dot_left(a, b, dims=NN):
    ah, al = halves(a)
    return dot(ah, b, dims) + dot(al, b, dims)


def sent_to_all(x, axis):
    copies = jnp.broadcast_to(x, (lax.axis_size(axis), *x.shape))
    return lax.all_to_all(copies, axis, split_axis=0, concat_axis=0, tiled=True)


def ring_gather(x, axis):
    n = lax.axis_size(axis)
    pieces = [x]
    for shift in (1, -1, -2):
        pieces.append(lax.ppermute(x, axis, [(i, (i + shift) % n) for i in range(n)]))
    return pieces


def places(index, n):
    return [index, lax.rem(index + n - 1, n), lax.rem(index + 1, n), lax.rem(index + 2, n)]


def fetches(core, across, near, mine_ref, other_ref, lanes, whole_ref, sems):
    copies = []
    for i, x in enumerate(across):
        for j, n in enumerate(near):
            for side, from_ref in enumerate((mine_ref, other_ref)):
                to = core if side == 0 else 1 - core
                copies.append(
                    pltpu.make_async_copy(
                        from_ref.at[i, j, :, :, lanes],
                        whole_ref.at[:, n, x, to],
                        sems.at[len(copies)],
                    )
                )
    return copies


def started(copies):
    for copy in copies:
        copy.start()


def finished(copies):
    for copy in copies:
        copy.wait()


def fade_rows(faded):
    high = faded.astype(BF).astype(F32)
    row = lax.broadcasted_iota(jnp.int32, (8, faded.shape[1]), 0)
    return jnp.where(row == 0, high, jnp.where(row == 1, faded - high, 0.0))


def fade_of(block):
    rows = block.shape[0]
    return block[rows - 8 : rows - 7] + block[rows - 7 : rows - 6]


def state_kernel(
    info_ref,
    own_ref,
    before_ref,
    after_ref,
    far_ref,
    gain_ref,
    mine_ref,
    other_ref,
    gap_ref,
    shift_ref,
    normed_out_ref,
    values_ref,
    opened_ref,
    cum_ref,
    growth_ref,
    payload_ref,
    whole_ref,
    sems,
    both_ref,
    tokens_ref,
    normed_ref,
    token_sems,
):
    rows, _ = normed_ref.shape
    cols = gap_ref.shape[1]
    block = own_ref.shape[0]
    spots = places(info_ref[1], rows // block)
    token_copies = [
        pltpu.make_async_copy(from_ref, tokens_ref.at[k], token_sems.at[k])
        for k, from_ref in enumerate((own_ref, before_ref, after_ref, far_ref))
    ]
    started(token_copies)
    copies = fetches(
        info_ref[0],
        range(mine_ref.shape[0]),
        range(mine_ref.shape[1]),
        mine_ref,
        other_ref,
        slice(None),
        whole_ref,
        sems,
    )
    started(copies)
    for k, spot in enumerate(spots):
        token_copies[k].wait()

        for i in range(block // 32):
            floats = tokens_ref[k, i * 32 : (i + 1) * 32, :].astype(F32)
            scale = lax.rsqrt(jnp.mean(floats * floats, axis=-1, keepdims=True) + EPSILON)
            at = pl.ds(pl.multiple_of(spot * block + i * 32, 32), 32)
            normed_ref[at, :] = (floats * scale * gain_ref[...]).astype(BF)
    handing = pltpu.make_async_copy(normed_ref, normed_out_ref, token_sems.at[len(spots)])
    handing.start()
    finished(copies)
    both_ref[...] = dot(normed_ref[...], whole_ref[...].reshape(-1, 2 * cols))
    row = lax.broadcasted_iota(jnp.int32, (CHUNK, CHUNK), 0)
    col = lax.broadcasted_iota(jnp.int32, (CHUNK, CHUNK), 1)
    tril = (row >= col).astype(BF)
    plane, height, _ = payload_ref.shape
    slab = height - 8
    for h in range(cols // RDIM):
        lanes = slice(h * RDIM, (h + 1) * RDIM)
        state = jnp.zeros((RDIM, RDIM), F32)
        faded = jnp.zeros((1, RDIM), F32)
        for c in range(rows // CHUNK):
            at = slice(c * CHUNK, (c + 1) * CHUNK)
            pre = both_ref[at, lanes].astype(BF).astype(F32)
            values = both_ref[at, cols + h * RDIM : cols + (h + 1) * RDIM].astype(BF)
            opened = gap_ref[:, lanes] / (1.0 + jnp.exp(pre))
            shift = jnp.broadcast_to(shift_ref[h : h + 1, at], (RDIM, CHUNK)).T
            decay = jnp.log1p(-opened) + shift
            d0, d1 = halves(decay)
            d2 = (decay - d0.astype(F32) - d1.astype(F32)).astype(BF)
            cum = dot(tril, d0) + (dot(tril, d1) + dot(tril, d2))
            total = cum[CHUNK - 1 :, :]
            growth = dot_left_t(values, opened * jnp.exp(total - cum))
            values_ref[at, lanes] = values
            opened_ref[at, lanes] = opened
            cum_ref[at, lanes] = cum
            growth_ref[c, :, lanes] = growth
            state = state * jnp.exp(total) + growth
            faded = faded + total
        fades = fade_rows(faded)
        for d in range(plane):
            block_d = jnp.concatenate([state[d * slab : (d + 1) * slab], fades], axis=0)
            payload_ref[d, :, lanes] = block_d.astype(BF)
    handing.wait()


def dot_left_t(values, key):
    kh, kl = halves(key)
    return dot(values, kh, TN) + dot(values, kl, TN)


def plane_kernel(got_ref, before_ref, faded_ref, total_ref):
    _, rows, cols = before_ref.shape
    state = jnp.zeros((rows, cols), F32)
    faded = jnp.zeros((1, cols), F32)
    for d in range(got_ref.shape[0]):
        got = got_ref[d].astype(F32)
        fade = fade_of(got)
        before_ref[d] = state
        faded_ref[d : d + 1, :] = faded
        state = state * jnp.exp(fade) + got[:rows]
        faded = faded + fade
    total = jnp.concatenate([state, fade_rows(faded)], axis=0).astype(BF)
    for z in range(total_ref.shape[0]):
        total_ref[z] = total


def depth_kernel(info_ref, totals_ref, before_ref, faded_ref, start_ref):
    planes = totals_ref.shape[0]
    devices, rows, cols = before_ref.shape
    state = jnp.zeros((rows, cols), F32)
    for z in range(planes):
        got = totals_ref[z].astype(F32)
        new = state * jnp.exp(fade_of(got)) + got[:rows]
        state = jnp.where(z < info_ref[4], new, state)
    for d in range(devices):
        start_ref[d] = (before_ref[d] + jnp.exp(faded_ref[d : d + 1, :]) * state).astype(BF)


def inner_kernel(
    info_ref,
    normed_ref,
    mine_ref,
    other_ref,
    values_ref,
    opened_ref,
    cum_ref,
    pooled_ref,
    decayed_ref,
    heard_ref,
    whole_ref,
    sems,
    both_ref,
    held_ref,
    held_sem,
):
    rows, cols = values_ref.shape
    bringing = pltpu.make_async_copy(normed_ref, held_ref, held_sem.at[0])
    bringing.start()
    copies = fetches(
        info_ref[0],
        places(info_ref[3], mine_ref.shape[0]),
        places(info_ref[5], mine_ref.shape[1]),
        mine_ref,
        other_ref,
        slice(0, 2 * cols),
        whole_ref,
        sems,
    )
    started(copies)
    finished(copies)
    bringing.wait()
    both_ref[...] = dot(held_ref[...], whole_ref[...].reshape(-1, 2 * cols))
    pooled_ref[...] = both_ref[:, cols:].astype(BF)
    row = lax.broadcasted_iota(jnp.int32, (CHUNK, CHUNK), 0)
    col = lax.broadcasted_iota(jnp.int32, (CHUNK, CHUNK), 1)
    for h in range(cols // RDIM):
        lanes = slice(h * RDIM, (h + 1) * RDIM)
        for c in range(rows // CHUNK):
            at = slice(c * CHUNK, (c + 1) * CHUNK)
            cum = cum_ref[at, lanes]
            query = both_ref[at, lanes].astype(BF).astype(F32) * jnp.exp(cum)
            key = opened_ref[at, lanes] * jnp.exp(-cum)
            scores = jnp.where(row >= col, dot_wide(query, key, NT), 0.0)
            decayed_ref[at, lanes] = query
            heard_ref[at, lanes] = dot_left(scores, values_ref[at, lanes])


def final_kernel(
    info_ref,
    start_ref,
    growth_ref,
    cum_ref,
    decayed_ref,
    heard_ref,
    pooled_ref,
    rim_ref,
    gain_ref,
    mine_ref,
    other_ref,
    part_ref,
    whole_ref,
    sems,
    mixed_ref,
):
    rows, cols = cum_ref.shape
    copies = fetches(
        info_ref[0],
        places(info_ref[3], mine_ref.shape[0]),
        places(info_ref[5], mine_ref.shape[1]),
        mine_ref,
        other_ref,
        slice(2 * cols, 4 * cols),
        whole_ref,
        sems,
    )
    started(copies)
    group = info_ref[1]
    padded = jnp.concatenate([rim_ref[...], pooled_ref[...]], axis=0).astype(F32)
    running = padded
    chosen = None
    for level in range(GROUPS):
        running = running + pltpu.roll(running, 2**level, 0)
        chosen = running if chosen is None else jnp.where(group == level, running, chosen)
    width = jnp.left_shift(jnp.int32(2), group)
    position = info_ref[2] + lax.broadcasted_iota(jnp.int32, (rows, cols), 0)
    divisor = jnp.minimum(position + 1, width).astype(F32)
    mixed_ref[:, :cols] = (chosen[RIM:] / divisor - padded[RIM:]).astype(BF)
    for h in range(cols // RDIM):
        lanes = slice(h * RDIM, (h + 1) * RDIM)
        state = start_ref[:, lanes].astype(F32)
        for c in range(rows // CHUNK):
            at = slice(c * CHUNK, (c + 1) * CHUNK)
            heard = heard_ref[at, lanes] + dot_wide(decayed_ref[at, lanes], state, NT)
            spread = lax.rsqrt(jnp.mean(heard * heard, axis=-1, keepdims=True) + EPSILON)
            mixed_ref[at, cols + h * RDIM : cols + (h + 1) * RDIM] = (
                heard * spread * gain_ref[...]
            ).astype(BF)
            total = cum_ref[(c + 1) * CHUNK - 1 : (c + 1) * CHUNK, lanes]
            state = state * jnp.exp(total) + growth_ref[c, :, lanes]

    finished(copies)
    far = whole_ref.shape[0]
    step = part_ref.shape[1] // far
    for f in range(far):
        weight = whole_ref[f].reshape(step, 2 * cols)
        part_ref[:, f * step : (f + 1) * step] = dot(mixed_ref[...], weight, NT).astype(BF)


VMEM = pl.BlockSpec(memory_space=pltpu.VMEM)
SMEM = pl.BlockSpec(memory_space=pltpu.SMEM)
HBM = pl.BlockSpec(memory_space=pltpu.HBM)


def spec_of(a):
    if a.dtype == jnp.int32:
        return SMEM
    return HBM if a.size * a.dtype.itemsize >= 1 << 19 and a.dtype == BF else VMEM


def call(kernel, outs, scratch, flops, moved, *args, out_specs=None):
    return pl.pallas_call(
        kernel,
        out_shape=outs,
        in_specs=[spec_of(a) for a in args],
        out_specs=out_specs or jax.tree.map(lambda _: VMEM, outs),
        scratch_shapes=scratch,
        cost_estimate=pl.CostEstimate(flops=flops, bytes_accessed=moved, transcendentals=0),
    )(*args)


def shape(dims, dtype):
    return jax.ShapeDtypeStruct(dims, dtype)


def side_by_side(*arrays):
    width = sum(a.shape[1] for a in arrays)
    total, at = None, 0
    for a in arrays:
        padded = jnp.pad(a, ((0, 0), (at, width - at - a.shape[1])))
        total = padded if total is None else total + padded
        at += a.shape[1]
    return total


def over_cores(x):
    return lax.ppermute(x, CORE, [(0, 1), (1, 0)])


def layer(
    tokens,
    norm_gain,
    pool_in_weight,
    query_weight,
    forget_weight,
    input_weight,
    forget_gap,
    decay_shift,
    out_gain,
    pool_out_weight,
    recur_out_weight,
):
    width = tokens.shape[1]
    cols = query_weight.shape[1]
    tp = lax.axis_size("tp")
    rows = tokens.shape[0] * tp
    devices = lax.axis_size(SP)
    info = jnp.stack(
        [
            lax.axis_index(CORE),
            lax.axis_index("tp"),
            lax.axis_index(SP) * rows,
            lax.axis_index(ACROSS),
            lax.axis_index(DEPTH),
            lax.axis_index(NEAR),
        ]
    ).astype(jnp.int32)

    pieces = ring_gather(tokens, "tp")
    weights = side_by_side(
        forget_weight,
        input_weight,
        query_weight,
        pool_in_weight,
        pool_out_weight.T,
        recur_out_weight.T,
    )
    weights = sent_to_all(weights, FAR)
    first = sent_to_all(weights[..., : 2 * cols], NEAR)
    first = sent_to_all(first, ACROSS)
    first_other = over_cores(first)
    rest = jnp.stack(ring_gather(weights[..., 2 * cols :], DEPTH))
    rest = jnp.stack(ring_gather(rest, ACROSS))
    rest_other = over_cores(rest)
    blocks = first.shape[2], first.shape[1], first.shape[0], 2, first.shape[3], 2 * cols
    whole = [
        pltpu.VMEM(blocks, BF),
        pltpu.SemaphoreType.DMA((2 * first.shape[0] * first.shape[1],)),
    ]

    plane = lax.axis_size(PLANE)
    slab = RDIM // plane
    normed, values, opened, cum, growth, payload = call(
        state_kernel,
        [
            shape((rows, width), BF),
            shape((rows, cols), BF),
            shape((rows, cols), F32),
            shape((rows, cols), F32),
            shape((rows // CHUNK, RDIM, cols), F32),
            shape((plane, slab + 8, cols), BF),
        ],
        [
            *whole,
            pltpu.VMEM((rows, 2 * cols), F32),
            pltpu.VMEM((tp, rows // tp, width), BF),
            pltpu.VMEM((rows, width), BF),
            pltpu.SemaphoreType.DMA((tp + 1,)),
        ],
        4 * rows * width * cols,
        8 << 20,
        info,
        *pieces,
        norm_gain[None, :],
        first,
        first_other,
        forget_gap[None, :],
        decay_shift,
        out_specs=[HBM, VMEM, VMEM, VMEM, VMEM, VMEM],
    )
    got = lax.all_to_all(payload, PLANE, split_axis=0, concat_axis=0, tiled=True)
    before, faded, total = call(
        plane_kernel,
        [
            shape((plane, slab, cols), F32),
            shape((plane, cols), F32),
            shape((lax.axis_size(DEPTH), slab + 8, cols), BF),
        ],
        [],
        1 << 20,
        1 << 19,
        got,
    )
    totals = lax.all_to_all(total, DEPTH, split_axis=0, concat_axis=0, tiled=True)
    start = call(
        depth_kernel,
        shape((plane, slab, cols), BF),
        [],
        1 << 20,
        1 << 19,
        info,
        totals,
        before,
        faded,
    )
    start = lax.all_to_all(
        start.reshape(RDIM, cols), PLANE, split_axis=0, concat_axis=0, tiled=True
    )
    pooled, decayed, heard = call(
        inner_kernel,
        [shape((rows, cols), BF), shape((rows, cols), F32), shape((rows, cols), F32)],
        [
            *whole,
            pltpu.VMEM((rows, 2 * cols), F32),
            pltpu.VMEM((rows, width), BF),
            pltpu.SemaphoreType.DMA((1,)),
        ],
        4 * rows * width * cols,
        8 << 20,
        info,
        normed,
        rest,
        rest_other,
        values,
        opened,
        cum,
    )
    order = [(i - 1, i) for i in range(1, devices)]
    rim = lax.ppermute(pooled[rows - RIM :], SP, order)
    part = call(
        final_kernel,
        shape((rows, width), BF),
        [*whole, pltpu.VMEM((rows, 2 * cols), BF)],
        4 * rows * width * cols,
        8 << 20,
        info,
        start,
        growth,
        cum,
        decayed,
        heard,
        pooled,
        rim,
        out_gain[None, :],
        rest,
        rest_other,
    )
    parts = lax.all_to_all(
        part.reshape(tp, rows // tp, width), "tp", split_axis=0, concat_axis=0, tiled=True
    )
    return jnp.sum(parts.astype(F32), axis=0).astype(BF)


def solution(mesh):
    split = Mesh(mesh.devices.reshape(4, 4, 4, 2, mesh.shape["tp"]), SP_TP)
    in_specs = (
        P(SP_TP, None),
        P(),
        P(SP, "tp"),
        P(SP, "tp"),
        P(SP, "tp"),
        P(SP, "tp"),
        P("tp"),
        P("tp", SP),
        P(),
        P("tp", SP),
        P("tp", SP),
    )
    out_specs = P(SP_TP, None)
    return jax.shard_map(layer, mesh=split, in_specs=in_specs, out_specs=out_specs, check_vma=False)
```

```python
import jax
import jax.numpy as jnp
from jax import lax
from jax.experimental import pallas as pl
from jax.experimental.pallas import tpu as pltpu
from jax.sharding import Mesh
from jax.sharding import PartitionSpec as P


GROUPS = 4
RDIM = 128
CHUNK = 128
RIM = 16
FAR, NEAR, ACROSS, CORE = "sp_f", "sp_n", "sp_x", "sp_c"
DEPTH = (FAR, NEAR)
PLANE = (ACROSS, CORE)
SP = (FAR, NEAR, ACROSS, CORE)
SP_TP = (FAR, NEAR, ACROSS, CORE, "tp")
EPSILON = 1e-06
BF = jnp.bfloat16
F32 = jnp.float32
NT = (((1,), (1,)), ((), ()))
TN = (((0,), (0,)), ((), ()))
NN = (((1,), (0,)), ((), ()))


def dot(a, b, dims=NN):
    return lax.dot_general(a, b, dims, preferred_element_type=F32)


def halves(x):
    high = x.astype(BF)
    return high, (x - high.astype(F32)).astype(BF)


def dot_wide(a, b, dims=NN):
    ah, al = halves(a)
    bh, bl = halves(b)
    return dot(ah, bh, dims) + (dot(ah, bl, dims) + dot(al, bh, dims))


def dot_left(a, b, dims=NN):
    ah, al = halves(a)
    return dot(ah, b, dims) + dot(al, b, dims)


def sent_to_all(x, axis):
    copies = jnp.broadcast_to(x, (lax.axis_size(axis), *x.shape))
    return lax.all_to_all(copies, axis, split_axis=0, concat_axis=0, tiled=True)


def ring_gather(x, axis):
    n = lax.axis_size(axis)
    pieces = [x]
    for shift in (1, -1, -2):
        pieces.append(lax.ppermute(x, axis, [(i, (i + shift) % n) for i in range(n)]))
    return pieces


def places(index, n):
    return [index, lax.rem(index + n - 1, n), lax.rem(index + 1, n), lax.rem(index + 2, n)]


def fetches(core, across, near, mine_ref, other_ref, lanes, whole_ref, sems):
    copies = []
    for i, x in enumerate(across):
        for j, n in enumerate(near):
            for side, from_ref in enumerate((mine_ref, other_ref)):
                to = core if side == 0 else 1 - core
                copies.append(
                    pltpu.make_async_copy(
                        from_ref.at[i, j, :, :, lanes],
                        whole_ref.at[:, n, x, to],
                        sems.at[len(copies)],
                    )
                )
    return copies


def started(copies):
    for copy in copies:
        copy.start()


def finished(copies):
    for copy in copies:
        copy.wait()


def fade_rows(faded):
    high = faded.astype(BF).astype(F32)
    row = lax.broadcasted_iota(jnp.int32, (8, faded.shape[1]), 0)
    return jnp.where(row == 0, high, jnp.where(row == 1, faded - high, 0.0))


def fade_of(block):
    rows = block.shape[0]
    return block[rows - 8 : rows - 7] + block[rows - 7 : rows - 6]


def state_kernel(
    info_ref,
    own_ref,
    before_ref,
    after_ref,
    far_ref,
    gain_ref,
    mine_ref,
    other_ref,
    gap_ref,
    shift_ref,
    normed_out_ref,
    values_ref,
    opened_ref,
    cum_ref,
    growth_ref,
    payload_ref,
    whole_ref,
    sems,
    both_ref,
    tokens_ref,
    normed_ref,
    token_sems,
):
    rows, _ = normed_ref.shape
    cols = gap_ref.shape[1]
    block = own_ref.shape[0]
    spots = places(info_ref[1], rows // block)
    token_copies = [
        pltpu.make_async_copy(from_ref, tokens_ref.at[k], token_sems.at[k])
        for k, from_ref in enumerate((own_ref, before_ref, after_ref, far_ref))
    ]
    started(token_copies)
    copies = fetches(
        info_ref[0],
        range(mine_ref.shape[0]),
        range(mine_ref.shape[1]),
        mine_ref,
        other_ref,
        slice(None),
        whole_ref,
        sems,
    )
    started(copies)
    for k, spot in enumerate(spots):
        token_copies[k].wait()

        for i in range(block // 32):
            floats = tokens_ref[k, i * 32 : (i + 1) * 32, :].astype(F32)
            scale = lax.rsqrt(jnp.mean(floats * floats, axis=-1, keepdims=True) + EPSILON)
            at = pl.ds(pl.multiple_of(spot * block + i * 32, 32), 32)
            normed_ref[at, :] = (floats * scale * gain_ref[...]).astype(BF)
    handing = pltpu.make_async_copy(normed_ref, normed_out_ref, token_sems.at[len(spots)])
    handing.start()
    finished(copies)
    both_ref[...] = dot(normed_ref[...], whole_ref[...].reshape(-1, 2 * cols))
    row = lax.broadcasted_iota(jnp.int32, (CHUNK, CHUNK), 0)
    col = lax.broadcasted_iota(jnp.int32, (CHUNK, CHUNK), 1)
    tril = (row >= col).astype(BF)
    plane, height, _ = payload_ref.shape
    slab = height - 8
    heads = cols // RDIM
    states = [jnp.zeros((RDIM, RDIM), F32) for _ in range(heads)]
    faded = jnp.zeros((1, cols), F32)
    for c in range(rows // CHUNK):
        at = slice(c * CHUNK, (c + 1) * CHUNK)
        pre = both_ref[at, :cols].astype(BF).astype(F32)
        values = both_ref[at, cols:].astype(BF)
        opened = gap_ref[...] / (1.0 + jnp.exp(pre))
        shift = jnp.concatenate(
            [jnp.broadcast_to(shift_ref[h : h + 1, at], (RDIM, CHUNK)).T for h in range(heads)],
            axis=1,
        )
        decay = jnp.log1p(-opened) + shift
        d0, d1 = halves(decay)
        d2 = (decay - d0.astype(F32) - d1.astype(F32)).astype(BF)
        cum = dot(tril, d0) + (dot(tril, d1) + dot(tril, d2))
        total = cum[CHUNK - 1 :, :]
        kept = jnp.exp(total)
        key = opened * jnp.exp(total - cum)
        values_ref[at, :] = values
        opened_ref[at, :] = opened
        cum_ref[at, :] = cum
        faded = faded + total
        for h in range(heads):
            lanes = slice(h * RDIM, (h + 1) * RDIM)
            growth = dot_left_t(values[:, lanes], key[:, lanes])
            growth_ref[c, :, lanes] = growth
            states[h] = states[h] * kept[:, lanes] + growth
    fades = fade_rows(faded)
    for h in range(heads):
        lanes = slice(h * RDIM, (h + 1) * RDIM)
        for d in range(plane):
            block_d = jnp.concatenate(
                [states[h][d * slab : (d + 1) * slab], fades[:, lanes]], axis=0
            )
            payload_ref[d, :, lanes] = block_d.astype(BF)
    handing.wait()


def dot_left_t(values, key):
    kh, kl = halves(key)
    return dot(values, kh, TN) + dot(values, kl, TN)


def plane_kernel(got_ref, before_ref, faded_ref, total_ref):
    _, rows, cols = before_ref.shape
    state = jnp.zeros((rows, cols), F32)
    faded = jnp.zeros((1, cols), F32)
    for d in range(got_ref.shape[0]):
        got = got_ref[d].astype(F32)
        fade = fade_of(got)
        before_ref[d] = state
        faded_ref[d : d + 1, :] = faded
        state = state * jnp.exp(fade) + got[:rows]
        faded = faded + fade
    total = jnp.concatenate([state, fade_rows(faded)], axis=0).astype(BF)
    for z in range(total_ref.shape[0]):
        total_ref[z] = total


def depth_kernel(info_ref, totals_ref, before_ref, faded_ref, start_ref):
    near, far = totals_ref.shape[:2]
    devices, rows, cols = before_ref.shape
    state = jnp.zeros((rows, cols), F32)
    for z in range(far * near):
        got = totals_ref[z % near, z // near].astype(F32)
        new = state * jnp.exp(fade_of(got)) + got[:rows]
        state = jnp.where(z < info_ref[4], new, state)
    for d in range(devices):
        start_ref[d] = (before_ref[d] + jnp.exp(faded_ref[d : d + 1, :]) * state).astype(BF)


def inner_kernel(
    info_ref,
    normed_ref,
    mine_ref,
    other_ref,
    values_ref,
    opened_ref,
    cum_ref,
    pooled_ref,
    edge_ref,
    decayed_ref,
    heard_ref,
    whole_ref,
    sems,
    both_ref,
    held_ref,
    held_sem,
):
    rows, cols = values_ref.shape
    bringing = pltpu.make_async_copy(normed_ref, held_ref, held_sem.at[0])
    bringing.start()
    copies = fetches(
        info_ref[0],
        places(info_ref[3], mine_ref.shape[0]),
        places(info_ref[5], mine_ref.shape[1]),
        mine_ref,
        other_ref,
        slice(0, 2 * cols),
        whole_ref,
        sems,
    )
    started(copies)
    finished(copies)
    bringing.wait()
    both_ref[...] = dot(held_ref[...], whole_ref[...].reshape(-1, 2 * cols))
    pooled_ref[...] = both_ref[:, cols:].astype(BF)
    edge_ref[...] = both_ref[rows - RIM :, cols:].astype(BF)
    row = lax.broadcasted_iota(jnp.int32, (CHUNK, CHUNK), 0)
    col = lax.broadcasted_iota(jnp.int32, (CHUNK, CHUNK), 1)
    for h in range(cols // RDIM):
        lanes = slice(h * RDIM, (h + 1) * RDIM)
        for c in range(rows // CHUNK):
            at = slice(c * CHUNK, (c + 1) * CHUNK)
            cum = cum_ref[at, lanes]
            query = both_ref[at, lanes].astype(BF).astype(F32) * jnp.exp(cum)
            key = opened_ref[at, lanes] * jnp.exp(-cum)
            scores = jnp.where(row >= col, dot_wide(query, key, NT), 0.0)
            decayed_ref[at, lanes] = query
            heard_ref[at, lanes] = dot_left(scores, values_ref[at, lanes])


def pool_kernel(info_ref, pooled_ref, rim_ref, pool_ref):
    rows, cols = pool_ref.shape
    group = info_ref[1]
    padded = jnp.concatenate([rim_ref[...], pooled_ref[...]], axis=0).astype(F32)
    running = padded
    chosen = None
    for level in range(GROUPS):
        running = running + pltpu.roll(running, 2**level, 0)
        chosen = running if chosen is None else jnp.where(group == level, running, chosen)
    width = jnp.left_shift(jnp.int32(2), group)
    position = info_ref[2] + lax.broadcasted_iota(jnp.int32, (rows, cols), 0)
    divisor = jnp.minimum(position + 1, width).astype(F32)
    pool_ref[...] = (chosen[RIM:] / divisor - padded[RIM:]).astype(BF)


def final_kernel(
    info_ref,
    start_ref,
    growth_ref,
    cum_ref,
    decayed_ref,
    heard_ref,
    pool_ref,
    gain_ref,
    mine_ref,
    other_ref,
    part_ref,
    whole_ref,
    sems,
    mixed_ref,
    held_ref,
    out_sems,
):
    rows, cols = cum_ref.shape
    copies = fetches(
        info_ref[0],
        places(info_ref[3], mine_ref.shape[0]),
        places(info_ref[5], mine_ref.shape[1]),
        mine_ref,
        other_ref,
        slice(2 * cols, 4 * cols),
        whole_ref,
        sems,
    )
    started(copies)
    mixed_ref[:, :cols] = pool_ref[...]
    for h in range(cols // RDIM):
        lanes = slice(h * RDIM, (h + 1) * RDIM)
        state = start_ref[:, lanes].astype(F32)
        for c in range(rows // CHUNK):
            at = slice(c * CHUNK, (c + 1) * CHUNK)
            heard = heard_ref[at, lanes] + dot_wide(decayed_ref[at, lanes], state, NT)
            spread = lax.rsqrt(jnp.mean(heard * heard, axis=-1, keepdims=True) + EPSILON)
            mixed_ref[at, cols + h * RDIM : cols + (h + 1) * RDIM] = (
                heard * spread * gain_ref[...]
            ).astype(BF)
            total = cum_ref[(c + 1) * CHUNK - 1 : (c + 1) * CHUNK, lanes]
            state = state * jnp.exp(total) + growth_ref[c, :, lanes]

    finished(copies)
    far = whole_ref.shape[0]
    step = part_ref.shape[1] // far
    leaving = []
    for f in range(far):
        weight = whole_ref[f].reshape(step, 2 * cols)
        held_ref[f] = dot(mixed_ref[...], weight, NT).astype(BF)
        leaving.append(
            pltpu.make_async_copy(
                held_ref.at[f], part_ref.at[:, pl.ds(f * step, step)], out_sems.at[f]
            )
        )
        leaving[-1].start()
    finished(leaving)


VMEM = pl.BlockSpec(memory_space=pltpu.VMEM)
SMEM = pl.BlockSpec(memory_space=pltpu.SMEM)
HBM = pl.BlockSpec(memory_space=pltpu.HBM)


def spec_of(a):
    if a.dtype == jnp.int32:
        return SMEM
    return HBM if a.size * a.dtype.itemsize >= 1 << 19 and a.dtype == BF else VMEM


def call(kernel, outs, scratch, flops, moved, *args, out_specs=None):
    return pl.pallas_call(
        kernel,
        out_shape=outs,
        in_specs=[spec_of(a) for a in args],
        out_specs=out_specs or jax.tree.map(lambda _: VMEM, outs),
        scratch_shapes=scratch,
        cost_estimate=pl.CostEstimate(flops=flops, bytes_accessed=moved, transcendentals=0),
    )(*args)


def shape(dims, dtype):
    return jax.ShapeDtypeStruct(dims, dtype)


def side_by_side(*arrays):
    width = sum(a.shape[1] for a in arrays)
    total, at = None, 0
    for a in arrays:
        padded = jnp.pad(a, ((0, 0), (at, width - at - a.shape[1])))
        total = padded if total is None else total + padded
        at += a.shape[1]
    return total


def over_cores(x):
    return lax.ppermute(x, CORE, [(0, 1), (1, 0)])


def layer(
    tokens,
    norm_gain,
    pool_in_weight,
    query_weight,
    forget_weight,
    input_weight,
    forget_gap,
    decay_shift,
    out_gain,
    pool_out_weight,
    recur_out_weight,
):
    width = tokens.shape[1]
    cols = query_weight.shape[1]
    tp = lax.axis_size("tp")
    rows = tokens.shape[0] * tp
    devices = lax.axis_size(SP)
    info = jnp.stack(
        [
            lax.axis_index(CORE),
            lax.axis_index("tp"),
            lax.axis_index(SP) * rows,
            lax.axis_index(ACROSS),
            lax.axis_index(DEPTH),
            lax.axis_index(NEAR),
        ]
    ).astype(jnp.int32)

    pieces = ring_gather(tokens, "tp")
    weights = side_by_side(
        forget_weight,
        input_weight,
        query_weight,
        pool_in_weight,
        pool_out_weight.T,
        recur_out_weight.T,
    )
    weights = sent_to_all(weights, FAR)
    first = sent_to_all(weights[..., : 2 * cols], NEAR)
    first = sent_to_all(first, ACROSS)
    first_other = over_cores(first)
    rest = jnp.stack(ring_gather(weights[..., 2 * cols :], DEPTH))
    rest = jnp.stack(ring_gather(rest, ACROSS))
    rest_other = over_cores(rest)
    blocks = first.shape[2], first.shape[1], first.shape[0], 2, first.shape[3], 2 * cols
    whole = [
        pltpu.VMEM(blocks, BF),
        pltpu.SemaphoreType.DMA((2 * first.shape[0] * first.shape[1],)),
    ]

    plane = lax.axis_size(PLANE)
    slab = RDIM // plane
    normed, values, opened, cum, growth, payload = call(
        state_kernel,
        [
            shape((rows, width), BF),
            shape((rows, cols), BF),
            shape((rows, cols), F32),
            shape((rows, cols), F32),
            shape((rows // CHUNK, RDIM, cols), F32),
            shape((plane, slab + 8, cols), BF),
        ],
        [
            *whole,
            pltpu.VMEM((rows, 2 * cols), F32),
            pltpu.VMEM((tp, rows // tp, width), BF),
            pltpu.VMEM((rows, width), BF),
            pltpu.SemaphoreType.DMA((tp + 1,)),
        ],
        4 * rows * width * cols,
        8 << 20,
        info,
        *pieces,
        norm_gain[None, :],
        first,
        first_other,
        forget_gap[None, :],
        decay_shift,
        out_specs=[HBM, VMEM, VMEM, VMEM, VMEM, VMEM],
    )
    got = lax.all_to_all(payload, PLANE, split_axis=0, concat_axis=0, tiled=True)
    before, faded, total = call(
        plane_kernel,
        [
            shape((plane, slab, cols), F32),
            shape((plane, cols), F32),
            shape((lax.axis_size(FAR), slab + 8, cols), BF),
        ],
        [],
        1 << 20,
        1 << 19,
        got,
    )
    totals = lax.all_to_all(total, FAR, split_axis=0, concat_axis=0, tiled=True)
    totals = sent_to_all(totals, NEAR)
    start = call(
        depth_kernel,
        shape((plane, slab, cols), BF),
        [],
        1 << 20,
        1 << 19,
        info,
        totals,
        before,
        faded,
    )
    start = lax.all_to_all(
        start.reshape(RDIM, cols), PLANE, split_axis=0, concat_axis=0, tiled=True
    )
    pooled, edge, decayed, heard = call(
        inner_kernel,
        [
            shape((rows, cols), BF),
            shape((RIM, cols), BF),
            shape((rows, cols), F32),
            shape((rows, cols), F32),
        ],
        [
            *whole,
            pltpu.VMEM((rows, 2 * cols), F32),
            pltpu.VMEM((rows, width), BF),
            pltpu.SemaphoreType.DMA((1,)),
        ],
        4 * rows * width * cols,
        8 << 20,
        info,
        normed,
        rest,
        rest_other,
        values,
        opened,
        cum,
    )
    order = [(i - 1, i) for i in range(1, devices)]
    rim = lax.ppermute(edge, SP, order)
    pool = call(pool_kernel, shape((rows, cols), BF), [], 1 << 20, 1 << 19, info, pooled, rim)
    part = call(
        final_kernel,
        shape((rows, width), BF),
        [
            *whole,
            pltpu.VMEM((rows, 2 * cols), BF),
            pltpu.VMEM((blocks[0], rows, width // blocks[0]), BF),
            pltpu.SemaphoreType.DMA((blocks[0],)),
        ],
        4 * rows * width * cols,
        8 << 20,
        info,
        start,
        growth,
        cum,
        decayed,
        heard,
        pool,
        out_gain[None, :],
        rest,
        rest_other,
        out_specs=HBM,
    )
    parts = lax.all_to_all(
        part.reshape(tp, rows // tp, width), "tp", split_axis=0, concat_axis=0, tiled=True
    )
    return jnp.sum(parts.astype(F32), axis=0).astype(BF)


def solution(mesh):
    split = Mesh(mesh.devices.reshape(4, 4, 4, 2, mesh.shape["tp"]), SP_TP)
    in_specs = (
        P(SP_TP, None),
        P(),
        P(SP, "tp"),
        P(SP, "tp"),
        P(SP, "tp"),
        P(SP, "tp"),
        P("tp"),
        P("tp", SP),
        P(),
        P("tp", SP),
        P("tp", SP),
    )
    out_specs = P(SP_TP, None)
    return jax.shard_map(layer, mesh=split, in_specs=in_specs, out_specs=out_specs, check_vma=False)
```

```python
import jax
import jax.numpy as jnp
from jax import lax
from jax.experimental import pallas as pl
from jax.experimental.pallas import tpu as pltpu
from jax.sharding import Mesh
from jax.sharding import PartitionSpec as P


GROUPS = 4
RDIM = 128
CHUNK = 128
RIM = 16
FAR, NEAR, ACROSS, CORE = "sp_f", "sp_n", "sp_x", "sp_c"
DEPTH = (FAR, NEAR)
PLANE = (ACROSS, CORE)
SP = (FAR, NEAR, ACROSS, CORE)
SP_TP = (FAR, NEAR, ACROSS, CORE, "tp")
EPSILON = 1e-06
BF = jnp.bfloat16
F32 = jnp.float32
NT = (((1,), (1,)), ((), ()))
TN = (((0,), (0,)), ((), ()))
NN = (((1,), (0,)), ((), ()))


def dot(a, b, dims=NN):
    return lax.dot_general(a, b, dims, preferred_element_type=F32)


def halves(x):
    high = x.astype(BF)
    return high, (x - high.astype(F32)).astype(BF)


def dot_wide(a, b, dims=NN):
    ah, al = halves(a)
    bh, bl = halves(b)
    return dot(ah, bh, dims) + (dot(ah, bl, dims) + dot(al, bh, dims))


def dot_left(a, b, dims=NN):
    ah, al = halves(a)
    return dot(ah, b, dims) + dot(al, b, dims)


def sent_to_all(x, axis):
    copies = jnp.broadcast_to(x, (lax.axis_size(axis), *x.shape))
    return lax.all_to_all(copies, axis, split_axis=0, concat_axis=0, tiled=True)


def ring_gather(x, axis):
    n = lax.axis_size(axis)
    pieces = [x]
    for shift in (1, -1, -2):
        pieces.append(lax.ppermute(x, axis, [(i, (i + shift) % n) for i in range(n)]))
    return pieces


def places(index, n):
    return [index, lax.rem(index + n - 1, n), lax.rem(index + 1, n), lax.rem(index + 2, n)]


def fetches(core, across, near, mine_ref, other_ref, lanes, whole_ref, sems):
    copies = []
    for i, x in enumerate(across):
        for j, n in enumerate(near):
            for side, from_ref in enumerate((mine_ref, other_ref)):
                to = core if side == 0 else 1 - core
                copies.append(
                    pltpu.make_async_copy(
                        from_ref.at[i, j, :, :, lanes],
                        whole_ref.at[:, n, x, to],
                        sems.at[len(copies)],
                    )
                )
    return copies


def started(copies):
    for copy in copies:
        copy.start()


def finished(copies):
    for copy in copies:
        copy.wait()


def fade_rows(faded):
    high = faded.astype(BF).astype(F32)
    row = lax.broadcasted_iota(jnp.int32, (8, faded.shape[1]), 0)
    return jnp.where(row == 0, high, jnp.where(row == 1, faded - high, 0.0))


def fade_of(block):
    rows = block.shape[0]
    return block[rows - 8 : rows - 7] + block[rows - 7 : rows - 6]


def state_kernel(
    info_ref,
    own_ref,
    before_ref,
    after_ref,
    far_ref,
    gain_ref,
    mine_ref,
    other_ref,
    gap_ref,
    shift_ref,
    normed_out_ref,
    values_ref,
    opened_ref,
    cum_ref,
    growth_ref,
    payload_ref,
    whole_ref,
    sems,
    both_ref,
    tokens_ref,
    normed_ref,
    token_sems,
):
    rows, _ = normed_ref.shape
    cols = gap_ref.shape[1]
    block = own_ref.shape[0]
    spots = places(info_ref[1], rows // block)
    token_copies = [
        pltpu.make_async_copy(from_ref, tokens_ref.at[k], token_sems.at[k])
        for k, from_ref in enumerate((own_ref, before_ref, after_ref, far_ref))
    ]
    started(token_copies)
    copies = fetches(
        info_ref[0],
        range(mine_ref.shape[0]),
        range(mine_ref.shape[1]),
        mine_ref,
        other_ref,
        slice(None),
        whole_ref,
        sems,
    )
    started(copies)
    for k, spot in enumerate(spots):
        token_copies[k].wait()

        for i in range(block // 32):
            floats = tokens_ref[k, i * 32 : (i + 1) * 32, :].astype(F32)
            scale = lax.rsqrt(jnp.mean(floats * floats, axis=-1, keepdims=True) + EPSILON)
            at = pl.ds(pl.multiple_of(spot * block + i * 32, 32), 32)
            normed_ref[at, :] = (floats * scale * gain_ref[...]).astype(BF)
    handing = pltpu.make_async_copy(normed_ref, normed_out_ref, token_sems.at[len(spots)])
    handing.start()
    finished(copies)
    both_ref[...] = dot(normed_ref[...], whole_ref[...].reshape(-1, 2 * cols))
    row = lax.broadcasted_iota(jnp.int32, (CHUNK, CHUNK), 0)
    col = lax.broadcasted_iota(jnp.int32, (CHUNK, CHUNK), 1)
    tril = (row >= col).astype(BF)
    plane, height, _ = payload_ref.shape
    slab = height - 8
    heads = cols // RDIM
    states = [jnp.zeros((RDIM, RDIM), F32) for _ in range(heads)]
    faded = jnp.zeros((1, cols), F32)
    for c in range(rows // CHUNK):
        at = slice(c * CHUNK, (c + 1) * CHUNK)
        pre = both_ref[at, :cols].astype(BF).astype(F32)
        values = both_ref[at, cols:].astype(BF)
        opened = gap_ref[...] / (1.0 + jnp.exp(pre))
        shift = jnp.concatenate(
            [jnp.broadcast_to(shift_ref[h : h + 1, at], (RDIM, CHUNK)).T for h in range(heads)],
            axis=1,
        )
        decay = jnp.log1p(-opened) + shift
        d0, d1 = halves(decay)
        d2 = (decay - d0.astype(F32) - d1.astype(F32)).astype(BF)
        cum = dot(tril, d0) + (dot(tril, d1) + dot(tril, d2))
        total = cum[CHUNK - 1 :, :]
        kept = jnp.exp(total)
        key = opened * jnp.exp(total - cum)
        values_ref[at, :] = values
        opened_ref[at, :] = opened
        cum_ref[at, :] = cum
        faded = faded + total
        for h in range(heads):
            lanes = slice(h * RDIM, (h + 1) * RDIM)
            growth = dot_left_t(values[:, lanes], key[:, lanes])
            growth_ref[c, :, lanes] = growth
            states[h] = states[h] * kept[:, lanes] + growth
    fades = fade_rows(faded)
    for h in range(heads):
        lanes = slice(h * RDIM, (h + 1) * RDIM)
        for d in range(plane):
            block_d = jnp.concatenate(
                [states[h][d * slab : (d + 1) * slab], fades[:, lanes]], axis=0
            )
            payload_ref[d, :, lanes] = block_d.astype(BF)
    handing.wait()


def dot_left_t(values, key):
    kh, kl = halves(key)
    return dot(values, kh, TN) + dot(values, kl, TN)


def plane_kernel(got_ref, before_ref, faded_ref, total_ref):
    _, rows, cols = before_ref.shape
    state = jnp.zeros((rows, cols), F32)
    faded = jnp.zeros((1, cols), F32)
    for d in range(got_ref.shape[0]):
        got = got_ref[d].astype(F32)
        fade = fade_of(got)
        before_ref[d] = state
        faded_ref[d : d + 1, :] = faded
        state = state * jnp.exp(fade) + got[:rows]
        faded = faded + fade
    total = jnp.concatenate([state, fade_rows(faded)], axis=0).astype(BF)
    for z in range(total_ref.shape[0]):
        total_ref[z] = total


def depth_kernel(info_ref, totals_ref, before_ref, faded_ref, start_ref):
    planes = totals_ref.shape[0]
    devices, rows, cols = before_ref.shape
    state = jnp.zeros((rows, cols), F32)
    for z in range(planes):
        got = totals_ref[z].astype(F32)
        new = state * jnp.exp(fade_of(got)) + got[:rows]
        state = jnp.where(z < info_ref[4], new, state)
    for d in range(devices):
        start_ref[d] = (before_ref[d] + jnp.exp(faded_ref[d : d + 1, :]) * state).astype(BF)


def inner_kernel(
    info_ref,
    normed_ref,
    mine_ref,
    other_ref,
    values_ref,
    opened_ref,
    cum_ref,
    pooled_ref,
    edge_ref,
    decayed_ref,
    heard_ref,
    whole_ref,
    sems,
    both_ref,
    held_ref,
    held_sem,
):
    rows, cols = values_ref.shape
    bringing = pltpu.make_async_copy(normed_ref, held_ref, held_sem.at[0])
    bringing.start()
    copies = fetches(
        info_ref[0],
        places(info_ref[3], mine_ref.shape[0]),
        places(info_ref[5], mine_ref.shape[1]),
        mine_ref,
        other_ref,
        slice(0, 2 * cols),
        whole_ref,
        sems,
    )
    started(copies)
    finished(copies)
    bringing.wait()
    both_ref[...] = dot(held_ref[...], whole_ref[...].reshape(-1, 2 * cols))
    pooled_ref[...] = both_ref[:, cols:].astype(BF)
    edge_ref[...] = both_ref[rows - RIM :, cols:].astype(BF)
    row = lax.broadcasted_iota(jnp.int32, (CHUNK, CHUNK), 0)
    col = lax.broadcasted_iota(jnp.int32, (CHUNK, CHUNK), 1)
    for h in range(cols // RDIM):
        lanes = slice(h * RDIM, (h + 1) * RDIM)
        for c in range(rows // CHUNK):
            at = slice(c * CHUNK, (c + 1) * CHUNK)
            cum = cum_ref[at, lanes]
            query = both_ref[at, lanes].astype(BF).astype(F32) * jnp.exp(cum)
            key = opened_ref[at, lanes] * jnp.exp(-cum)
            scores = jnp.where(row >= col, dot_wide(query, key, NT), 0.0)
            decayed_ref[at, lanes] = query
            heard_ref[at, lanes] = dot_left(scores, values_ref[at, lanes])


def pool_kernel(info_ref, pooled_ref, rim_ref, pool_ref):
    rows, cols = pool_ref.shape
    group = info_ref[1]
    padded = jnp.concatenate([rim_ref[...], pooled_ref[...]], axis=0).astype(F32)
    running = padded
    chosen = None
    for level in range(GROUPS):
        running = running + pltpu.roll(running, 2**level, 0)
        chosen = running if chosen is None else jnp.where(group == level, running, chosen)
    width = jnp.left_shift(jnp.int32(2), group)
    position = info_ref[2] + lax.broadcasted_iota(jnp.int32, (rows, cols), 0)
    divisor = jnp.minimum(position + 1, width).astype(F32)
    pool_ref[...] = (chosen[RIM:] / divisor - padded[RIM:]).astype(BF)


def final_kernel(
    info_ref,
    start_ref,
    growth_ref,
    cum_ref,
    decayed_ref,
    heard_ref,
    pool_ref,
    gain_ref,
    mine_ref,
    other_ref,
    part_ref,
    whole_ref,
    sems,
    mixed_ref,
    held_ref,
    out_sems,
):
    rows, cols = cum_ref.shape
    copies = fetches(
        info_ref[0],
        places(info_ref[3], mine_ref.shape[0]),
        places(info_ref[5], mine_ref.shape[1]),
        mine_ref,
        other_ref,
        slice(2 * cols, 4 * cols),
        whole_ref,
        sems,
    )
    started(copies)
    mixed_ref[:, :cols] = pool_ref[...]
    for h in range(cols // RDIM):
        lanes = slice(h * RDIM, (h + 1) * RDIM)
        state = start_ref[:, lanes].astype(F32)
        for c in range(rows // CHUNK):
            at = slice(c * CHUNK, (c + 1) * CHUNK)
            heard = heard_ref[at, lanes] + dot_wide(decayed_ref[at, lanes], state, NT)
            spread = lax.rsqrt(jnp.mean(heard * heard, axis=-1, keepdims=True) + EPSILON)
            mixed_ref[at, cols + h * RDIM : cols + (h + 1) * RDIM] = (
                heard * spread * gain_ref[...]
            ).astype(BF)
            total = cum_ref[(c + 1) * CHUNK - 1 : (c + 1) * CHUNK, lanes]
            state = state * jnp.exp(total) + growth_ref[c, :, lanes]

    finished(copies)
    far = whole_ref.shape[0]
    step = part_ref.shape[1] // far
    leaving = []
    for f in range(far):
        weight = whole_ref[f].reshape(step, 2 * cols)
        held_ref[f] = dot(mixed_ref[...], weight, NT).astype(BF)
        leaving.append(
            pltpu.make_async_copy(
                held_ref.at[f], part_ref.at[:, pl.ds(f * step, step)], out_sems.at[f]
            )
        )
        leaving[-1].start()
    finished(leaving)


VMEM = pl.BlockSpec(memory_space=pltpu.VMEM)
SMEM = pl.BlockSpec(memory_space=pltpu.SMEM)
HBM = pl.BlockSpec(memory_space=pltpu.HBM)


def spec_of(a):
    if a.dtype == jnp.int32:
        return SMEM
    return HBM if a.size * a.dtype.itemsize >= 1 << 19 and a.dtype == BF else VMEM


def call(kernel, outs, scratch, flops, moved, *args, out_specs=None):
    return pl.pallas_call(
        kernel,
        out_shape=outs,
        in_specs=[spec_of(a) for a in args],
        out_specs=out_specs or jax.tree.map(lambda _: VMEM, outs),
        scratch_shapes=scratch,
        cost_estimate=pl.CostEstimate(flops=flops, bytes_accessed=moved, transcendentals=0),
    )(*args)


def shape(dims, dtype):
    return jax.ShapeDtypeStruct(dims, dtype)


def side_by_side(*arrays):
    width = sum(a.shape[1] for a in arrays)
    total, at = None, 0
    for a in arrays:
        padded = jnp.pad(a, ((0, 0), (at, width - at - a.shape[1])))
        total = padded if total is None else total + padded
        at += a.shape[1]
    return total


def over_cores(x):
    return lax.ppermute(x, CORE, [(0, 1), (1, 0)])


def layer(
    tokens,
    norm_gain,
    pool_in_weight,
    query_weight,
    forget_weight,
    input_weight,
    forget_gap,
    decay_shift,
    out_gain,
    pool_out_weight,
    recur_out_weight,
):
    width = tokens.shape[1]
    cols = query_weight.shape[1]
    tp = lax.axis_size("tp")
    rows = tokens.shape[0] * tp
    devices = lax.axis_size(SP)
    info = jnp.stack(
        [
            lax.axis_index(CORE),
            lax.axis_index("tp"),
            lax.axis_index(SP) * rows,
            lax.axis_index(ACROSS),
            lax.axis_index(DEPTH),
            lax.axis_index(NEAR),
        ]
    ).astype(jnp.int32)

    pieces = ring_gather(tokens, "tp")
    weights = side_by_side(
        forget_weight,
        input_weight,
        query_weight,
        pool_in_weight,
        pool_out_weight.T,
        recur_out_weight.T,
    )
    weights = sent_to_all(weights, FAR)
    first = sent_to_all(weights[..., : 2 * cols], NEAR)
    first = sent_to_all(first, ACROSS)
    first_other = over_cores(first)
    rest = jnp.stack(ring_gather(weights[..., 2 * cols :], DEPTH))
    rest = jnp.stack(ring_gather(rest, ACROSS))
    rest_other = over_cores(rest)
    blocks = first.shape[2], first.shape[1], first.shape[0], 2, first.shape[3], 2 * cols
    whole = [
        pltpu.VMEM(blocks, BF),
        pltpu.SemaphoreType.DMA((2 * first.shape[0] * first.shape[1],)),
    ]

    plane = lax.axis_size(PLANE)
    slab = RDIM // plane
    normed, values, opened, cum, growth, payload = call(
        state_kernel,
        [
            shape((rows, width), BF),
            shape((rows, cols), BF),
            shape((rows, cols), F32),
            shape((rows, cols), F32),
            shape((rows // CHUNK, RDIM, cols), F32),
            shape((plane, slab + 8, cols), BF),
        ],
        [
            *whole,
            pltpu.VMEM((rows, 2 * cols), F32),
            pltpu.VMEM((tp, rows // tp, width), BF),
            pltpu.VMEM((rows, width), BF),
            pltpu.SemaphoreType.DMA((tp + 1,)),
        ],
        4 * rows * width * cols,
        8 << 20,
        info,
        *pieces,
        norm_gain[None, :],
        first,
        first_other,
        forget_gap[None, :],
        decay_shift,
        out_specs=[HBM, VMEM, VMEM, VMEM, VMEM, VMEM],
    )
    got = lax.all_to_all(payload, PLANE, split_axis=0, concat_axis=0, tiled=True)
    before, faded, total = call(
        plane_kernel,
        [
            shape((plane, slab, cols), F32),
            shape((plane, cols), F32),
            shape((lax.axis_size(DEPTH), slab + 8, cols), BF),
        ],
        [],
        1 << 20,
        1 << 19,
        got,
    )
    totals = lax.all_to_all(total, DEPTH, split_axis=0, concat_axis=0, tiled=True)
    start = call(
        depth_kernel,
        shape((plane, slab, cols), BF),
        [],
        1 << 20,
        1 << 19,
        info,
        totals,
        before,
        faded,
    )
    start = lax.all_to_all(
        start.reshape(RDIM, cols), PLANE, split_axis=0, concat_axis=0, tiled=True
    )
    pooled, edge, decayed, heard = call(
        inner_kernel,
        [
            shape((rows, cols), BF),
            shape((RIM, cols), BF),
            shape((rows, cols), F32),
            shape((rows, cols), F32),
        ],
        [
            *whole,
            pltpu.VMEM((rows, 2 * cols), F32),
            pltpu.VMEM((rows, width), BF),
            pltpu.SemaphoreType.DMA((1,)),
        ],
        4 * rows * width * cols,
        8 << 20,
        info,
        normed,
        rest,
        rest_other,
        values,
        opened,
        cum,
    )
    order = [(i - 1, i) for i in range(1, devices)]
    rim = lax.ppermute(edge, SP, order)
    pool = call(pool_kernel, shape((rows, cols), BF), [], 1 << 20, 1 << 19, info, pooled, rim)
    part = call(
        final_kernel,
        shape((rows, width), BF),
        [
            *whole,
            pltpu.VMEM((rows, 2 * cols), BF),
            pltpu.VMEM((blocks[0], rows, width // blocks[0]), BF),
            pltpu.SemaphoreType.DMA((blocks[0],)),
        ],
        4 * rows * width * cols,
        8 << 20,
        info,
        start,
        growth,
        cum,
        decayed,
        heard,
        pool,
        out_gain[None, :],
        rest,
        rest_other,
        out_specs=HBM,
    )
    parts = lax.all_to_all(
        part.reshape(tp, rows // tp, width), "tp", split_axis=0, concat_axis=0, tiled=True
    )
    return jnp.sum(parts.astype(F32), axis=0).astype(BF)


def solution(mesh):
    split = Mesh(mesh.devices.reshape(4, 4, 4, 2, mesh.shape["tp"]), SP_TP)
    in_specs = (
        P(SP_TP, None),
        P(),
        P(SP, "tp"),
        P(SP, "tp"),
        P(SP, "tp"),
        P(SP, "tp"),
        P("tp"),
        P("tp", SP),
        P(),
        P("tp", SP),
        P("tp", SP),
    )
    out_specs = P(SP_TP, None)
    return jax.shard_map(layer, mesh=split, in_specs=in_specs, out_specs=out_specs, check_vma=False)
```

```python
import jax
import jax.numpy as jnp
from jax import lax
from jax.experimental import pallas as pl
from jax.experimental.pallas import tpu as pltpu
from jax.sharding import Mesh
from jax.sharding import PartitionSpec as P


GROUPS = 4
RDIM = 128
CHUNK = 128
RIM = 16
FAR, NEAR, ACROSS, CORE = "sp_f", "sp_n", "sp_x", "sp_c"
DEPTH = (FAR, NEAR)
PLANE = (ACROSS, CORE)
SP = (FAR, NEAR, ACROSS, CORE)
SP_TP = (FAR, NEAR, ACROSS, CORE, "tp")
EPSILON = 1e-06
BF = jnp.bfloat16
F32 = jnp.float32
NT = (((1,), (1,)), ((), ()))
TN = (((0,), (0,)), ((), ()))
NN = (((1,), (0,)), ((), ()))


def dot(a, b, dims=NN):
    return lax.dot_general(a, b, dims, preferred_element_type=F32)


def halves(x):
    high = x.astype(BF)
    return high, (x - high.astype(F32)).astype(BF)


def dot_wide(a, b, dims=NN):
    ah, al = halves(a)
    bh, bl = halves(b)
    return dot(ah, bh, dims) + (dot(ah, bl, dims) + dot(al, bh, dims))


def dot_left(a, b, dims=NN):
    ah, al = halves(a)
    return dot(ah, b, dims) + dot(al, b, dims)


def sent_to_all(x, axis):
    copies = jnp.broadcast_to(x, (lax.axis_size(axis), *x.shape))
    return lax.all_to_all(copies, axis, split_axis=0, concat_axis=0, tiled=True)


def ring_gather(x, axis):
    n = lax.axis_size(axis)
    pieces = [x]
    for shift in (1, -1, -2):
        pieces.append(lax.ppermute(x, axis, [(i, (i + shift) % n) for i in range(n)]))
    return pieces


def places(index, n):
    return [index, lax.rem(index + n - 1, n), lax.rem(index + 1, n), lax.rem(index + 2, n)]


def fetches(core, across, near, mine_ref, other_ref, lanes, whole_ref, sems):
    copies = []
    for i, x in enumerate(across):
        for j, n in enumerate(near):
            for side, from_ref in enumerate((mine_ref, other_ref)):
                to = core if side == 0 else 1 - core
                copies.append(
                    pltpu.make_async_copy(
                        from_ref.at[i, j, :, :, lanes],
                        whole_ref.at[:, n, x, to],
                        sems.at[len(copies)],
                    )
                )
    return copies


def started(copies):
    for copy in copies:
        copy.start()


def finished(copies):
    for copy in copies:
        copy.wait()


def fade_rows(faded):
    high = faded.astype(BF).astype(F32)
    row = lax.broadcasted_iota(jnp.int32, (8, faded.shape[1]), 0)
    return jnp.where(row == 0, high, jnp.where(row == 1, faded - high, 0.0))


def fade_of(block):
    rows = block.shape[0]
    return block[rows - 8 : rows - 7] + block[rows - 7 : rows - 6]


def state_kernel(
    info_ref,
    own_ref,
    before_ref,
    after_ref,
    far_ref,
    gain_ref,
    mine_ref,
    other_ref,
    gap_ref,
    shift_ref,
    normed_out_ref,
    values_ref,
    opened_ref,
    cum_ref,
    growth_ref,
    payload_ref,
    edge_ref,
    whole_ref,
    sems,
    both_ref,
    tokens_ref,
    normed_ref,
    token_sems,
):
    rows, _ = normed_ref.shape
    cols = gap_ref.shape[1]
    block = own_ref.shape[0]
    spots = places(info_ref[1], rows // block)
    token_copies = [
        pltpu.make_async_copy(from_ref, tokens_ref.at[k], token_sems.at[k])
        for k, from_ref in enumerate((own_ref, before_ref, after_ref, far_ref))
    ]
    started(token_copies)
    copies = fetches(
        info_ref[0],
        range(mine_ref.shape[0]),
        range(mine_ref.shape[1]),
        mine_ref,
        other_ref,
        slice(None),
        whole_ref,
        sems,
    )
    started(copies)
    for k, spot in enumerate(spots):
        token_copies[k].wait()

        for i in range(block // 32):
            floats = tokens_ref[k, i * 32 : (i + 1) * 32, :].astype(F32)
            scale = lax.rsqrt(jnp.mean(floats * floats, axis=-1, keepdims=True) + EPSILON)
            at = pl.ds(pl.multiple_of(spot * block + i * 32, 32), 32)
            normed_ref[at, :] = (floats * scale * gain_ref[...]).astype(BF)
    handing = pltpu.make_async_copy(normed_ref, normed_out_ref, token_sems.at[len(spots)])
    handing.start()
    edge_ref[...] = normed_ref[rows - RIM :, :]
    finished(copies)
    both_ref[...] = dot(normed_ref[...], whole_ref[...].reshape(-1, 2 * cols))
    row = lax.broadcasted_iota(jnp.int32, (CHUNK, CHUNK), 0)
    col = lax.broadcasted_iota(jnp.int32, (CHUNK, CHUNK), 1)
    tril = (row >= col).astype(BF)
    plane, height, _ = payload_ref.shape
    slab = height - 8
    heads = cols // RDIM
    states = [jnp.zeros((RDIM, RDIM), F32) for _ in range(heads)]
    faded = jnp.zeros((1, cols), F32)
    for c in range(rows // CHUNK):
        at = slice(c * CHUNK, (c + 1) * CHUNK)
        pre = both_ref[at, :cols].astype(BF).astype(F32)
        values = both_ref[at, cols:].astype(BF)
        opened = gap_ref[...] / (1.0 + jnp.exp(pre))
        shift = jnp.concatenate(
            [jnp.broadcast_to(shift_ref[h : h + 1, at], (RDIM, CHUNK)).T for h in range(heads)],
            axis=1,
        )
        decay = jnp.log1p(-opened) + shift
        d0, d1 = halves(decay)
        d2 = (decay - d0.astype(F32) - d1.astype(F32)).astype(BF)
        cum = dot(tril, d0) + (dot(tril, d1) + dot(tril, d2))
        total = cum[CHUNK - 1 :, :]
        kept = jnp.exp(total)
        key = opened * jnp.exp(total - cum)
        values_ref[at, :] = values
        opened_ref[at, :] = opened
        cum_ref[at, :] = cum
        faded = faded + total
        for h in range(heads):
            lanes = slice(h * RDIM, (h + 1) * RDIM)
            growth = dot_left_t(values[:, lanes], key[:, lanes])
            growth_ref[c, :, lanes] = growth
            states[h] = states[h] * kept[:, lanes] + growth
    fades = fade_rows(faded)
    for h in range(heads):
        lanes = slice(h * RDIM, (h + 1) * RDIM)
        for d in range(plane):
            block_d = jnp.concatenate(
                [states[h][d * slab : (d + 1) * slab], fades[:, lanes]], axis=0
            )
            payload_ref[d, :, lanes] = block_d.astype(BF)
    handing.wait()


def dot_left_t(values, key):
    kh, kl = halves(key)
    return dot(values, kh, TN) + dot(values, kl, TN)


def plane_kernel(got_ref, before_ref, faded_ref, total_ref):
    _, rows, cols = before_ref.shape
    state = jnp.zeros((rows, cols), F32)
    faded = jnp.zeros((1, cols), F32)
    for d in range(got_ref.shape[0]):
        got = got_ref[d].astype(F32)
        fade = fade_of(got)
        before_ref[d] = state
        faded_ref[d : d + 1, :] = faded
        state = state * jnp.exp(fade) + got[:rows]
        faded = faded + fade
    total = jnp.concatenate([state, fade_rows(faded)], axis=0).astype(BF)
    for z in range(total_ref.shape[0]):
        total_ref[z] = total


def depth_kernel(info_ref, totals_ref, before_ref, faded_ref, start_ref):
    planes = totals_ref.shape[0]
    devices, rows, cols = before_ref.shape
    state = jnp.zeros((rows, cols), F32)
    for z in range(planes):
        got = totals_ref[z].astype(F32)
        new = state * jnp.exp(fade_of(got)) + got[:rows]
        state = jnp.where(z < info_ref[4], new, state)
    for d in range(devices):
        start_ref[d] = (before_ref[d] + jnp.exp(faded_ref[d : d + 1, :]) * state).astype(BF)


def inner_kernel(
    info_ref,
    normed_ref,
    mine_ref,
    other_ref,
    values_ref,
    opened_ref,
    cum_ref,
    rim_ref,
    pooled_ref,
    edge_ref,
    decayed_ref,
    heard_ref,
    whole_ref,
    sems,
    both_ref,
    held_ref,
    held_sem,
):
    rows, cols = values_ref.shape
    bringing = pltpu.make_async_copy(normed_ref, held_ref, held_sem.at[0])
    bringing.start()
    copies = fetches(
        info_ref[0],
        places(info_ref[3], mine_ref.shape[0]),
        places(info_ref[5], mine_ref.shape[1]),
        mine_ref,
        other_ref,
        slice(0, 2 * cols),
        whole_ref,
        sems,
    )
    started(copies)
    finished(copies)
    bringing.wait()
    both_ref[...] = dot(held_ref[...], whole_ref[...].reshape(-1, 2 * cols))
    pooled_ref[...] = both_ref[:, cols:].astype(BF)
    edge_ref[...] = dot(rim_ref[...], whole_ref[..., cols:].reshape(-1, cols)).astype(BF)
    row = lax.broadcasted_iota(jnp.int32, (CHUNK, CHUNK), 0)
    col = lax.broadcasted_iota(jnp.int32, (CHUNK, CHUNK), 1)
    for h in range(cols // RDIM):
        lanes = slice(h * RDIM, (h + 1) * RDIM)
        for c in range(rows // CHUNK):
            at = slice(c * CHUNK, (c + 1) * CHUNK)
            cum = cum_ref[at, lanes]
            query = both_ref[at, lanes].astype(BF).astype(F32) * jnp.exp(cum)
            key = opened_ref[at, lanes] * jnp.exp(-cum)
            scores = jnp.where(row >= col, dot_wide(query, key, NT), 0.0)
            decayed_ref[at, lanes] = query
            heard_ref[at, lanes] = dot_left(scores, values_ref[at, lanes])


def pool_kernel(info_ref, pooled_ref, rim_ref, pool_ref):
    rows, cols = pool_ref.shape
    group = info_ref[1]
    padded = jnp.concatenate([rim_ref[...], pooled_ref[...]], axis=0).astype(F32)
    running = padded
    chosen = None
    for level in range(GROUPS):
        running = running + pltpu.roll(running, 2**level, 0)
        chosen = running if chosen is None else jnp.where(group == level, running, chosen)
    width = jnp.left_shift(jnp.int32(2), group)
    position = info_ref[2] + lax.broadcasted_iota(jnp.int32, (rows, cols), 0)
    divisor = jnp.minimum(position + 1, width).astype(F32)
    pool_ref[...] = (chosen[RIM:] / divisor - padded[RIM:]).astype(BF)


def final_kernel(
    info_ref,
    start_ref,
    growth_ref,
    cum_ref,
    decayed_ref,
    heard_ref,
    pool_ref,
    gain_ref,
    mine_ref,
    other_ref,
    part_ref,
    whole_ref,
    sems,
    mixed_ref,
    held_ref,
    out_sems,
):
    rows, cols = cum_ref.shape
    copies = fetches(
        info_ref[0],
        places(info_ref[3], mine_ref.shape[0]),
        places(info_ref[5], mine_ref.shape[1]),
        mine_ref,
        other_ref,
        slice(2 * cols, 4 * cols),
        whole_ref,
        sems,
    )
    started(copies)
    mixed_ref[:, :cols] = pool_ref[...]
    for h in range(cols // RDIM):
        lanes = slice(h * RDIM, (h + 1) * RDIM)
        state = start_ref[:, lanes].astype(F32)
        for c in range(rows // CHUNK):
            at = slice(c * CHUNK, (c + 1) * CHUNK)
            heard = heard_ref[at, lanes] + dot_wide(decayed_ref[at, lanes], state, NT)
            spread = lax.rsqrt(jnp.mean(heard * heard, axis=-1, keepdims=True) + EPSILON)
            mixed_ref[at, cols + h * RDIM : cols + (h + 1) * RDIM] = (
                heard * spread * gain_ref[...]
            ).astype(BF)
            total = cum_ref[(c + 1) * CHUNK - 1 : (c + 1) * CHUNK, lanes]
            state = state * jnp.exp(total) + growth_ref[c, :, lanes]

    finished(copies)
    far = whole_ref.shape[0]
    step = part_ref.shape[1] // far
    leaving = []
    for f in range(far):
        weight = whole_ref[f].reshape(step, 2 * cols)
        held_ref[f] = dot(mixed_ref[...], weight, NT).astype(BF)
        leaving.append(
            pltpu.make_async_copy(
                held_ref.at[f], part_ref.at[:, pl.ds(f * step, step)], out_sems.at[f]
            )
        )
        leaving[-1].start()
    finished(leaving)


VMEM = pl.BlockSpec(memory_space=pltpu.VMEM)
SMEM = pl.BlockSpec(memory_space=pltpu.SMEM)
HBM = pl.BlockSpec(memory_space=pltpu.HBM)


def spec_of(a):
    if a.dtype == jnp.int32:
        return SMEM
    return HBM if a.size * a.dtype.itemsize >= 1 << 19 and a.dtype == BF else VMEM


def call(kernel, outs, scratch, flops, moved, *args, out_specs=None):
    return pl.pallas_call(
        kernel,
        out_shape=outs,
        in_specs=[spec_of(a) for a in args],
        out_specs=out_specs or jax.tree.map(lambda _: VMEM, outs),
        scratch_shapes=scratch,
        cost_estimate=pl.CostEstimate(flops=flops, bytes_accessed=moved, transcendentals=0),
    )(*args)


def shape(dims, dtype):
    return jax.ShapeDtypeStruct(dims, dtype)


def side_by_side(*arrays):
    width = sum(a.shape[1] for a in arrays)
    total, at = None, 0
    for a in arrays:
        padded = jnp.pad(a, ((0, 0), (at, width - at - a.shape[1])))
        total = padded if total is None else total + padded
        at += a.shape[1]
    return total


def over_cores(x):
    return lax.ppermute(x, CORE, [(0, 1), (1, 0)])


def layer(
    tokens,
    norm_gain,
    pool_in_weight,
    query_weight,
    forget_weight,
    input_weight,
    forget_gap,
    decay_shift,
    out_gain,
    pool_out_weight,
    recur_out_weight,
):
    width = tokens.shape[1]
    cols = query_weight.shape[1]
    tp = lax.axis_size("tp")
    rows = tokens.shape[0] * tp
    devices = lax.axis_size(SP)
    info = jnp.stack(
        [
            lax.axis_index(CORE),
            lax.axis_index("tp"),
            lax.axis_index(SP) * rows,
            lax.axis_index(ACROSS),
            lax.axis_index(DEPTH),
            lax.axis_index(NEAR),
        ]
    ).astype(jnp.int32)

    pieces = ring_gather(tokens, "tp")
    weights = side_by_side(
        forget_weight,
        input_weight,
        query_weight,
        pool_in_weight,
        pool_out_weight.T,
        recur_out_weight.T,
    )
    weights = sent_to_all(weights, FAR)
    first = sent_to_all(weights[..., : 2 * cols], NEAR)
    first = sent_to_all(first, ACROSS)
    first_other = over_cores(first)
    rest = jnp.stack(ring_gather(weights[..., 2 * cols :], DEPTH))
    rest = jnp.stack(ring_gather(rest, ACROSS))
    rest_other = over_cores(rest)
    blocks = first.shape[2], first.shape[1], first.shape[0], 2, first.shape[3], 2 * cols
    whole = [
        pltpu.VMEM(blocks, BF),
        pltpu.SemaphoreType.DMA((2 * first.shape[0] * first.shape[1],)),
    ]

    plane = lax.axis_size(PLANE)
    slab = RDIM // plane
    normed, values, opened, cum, growth, payload, edge = call(
        state_kernel,
        [
            shape((rows, width), BF),
            shape((rows, cols), BF),
            shape((rows, cols), F32),
            shape((rows, cols), F32),
            shape((rows // CHUNK, RDIM, cols), F32),
            shape((plane, slab + 8, cols), BF),
            shape((RIM, width), BF),
        ],
        [
            *whole,
            pltpu.VMEM((rows, 2 * cols), F32),
            pltpu.VMEM((tp, rows // tp, width), BF),
            pltpu.VMEM((rows, width), BF),
            pltpu.SemaphoreType.DMA((tp + 1,)),
        ],
        4 * rows * width * cols,
        8 << 20,
        info,
        *pieces,
        norm_gain[None, :],
        first,
        first_other,
        forget_gap[None, :],
        decay_shift,
        out_specs=[HBM, VMEM, VMEM, VMEM, VMEM, VMEM, VMEM],
    )
    order = [(i - 1, i) for i in range(1, devices)]
    rim = lax.ppermute(edge, SP, order)
    got = lax.all_to_all(payload, PLANE, split_axis=0, concat_axis=0, tiled=True)
    before, faded, total = call(
        plane_kernel,
        [
            shape((plane, slab, cols), F32),
            shape((plane, cols), F32),
            shape((lax.axis_size(DEPTH), slab + 8, cols), BF),
        ],
        [],
        1 << 20,
        1 << 19,
        got,
    )
    totals = lax.all_to_all(total, DEPTH, split_axis=0, concat_axis=0, tiled=True)
    start = call(
        depth_kernel,
        shape((plane, slab, cols), BF),
        [],
        1 << 20,
        1 << 19,
        info,
        totals,
        before,
        faded,
    )
    start = lax.all_to_all(
        start.reshape(RDIM, cols), PLANE, split_axis=0, concat_axis=0, tiled=True
    )
    pooled, before_pooled, decayed, heard = call(
        inner_kernel,
        [
            shape((rows, cols), BF),
            shape((RIM, cols), BF),
            shape((rows, cols), F32),
            shape((rows, cols), F32),
        ],
        [
            *whole,
            pltpu.VMEM((rows, 2 * cols), F32),
            pltpu.VMEM((rows, width), BF),
            pltpu.SemaphoreType.DMA((1,)),
        ],
        4 * rows * width * cols,
        8 << 20,
        info,
        normed,
        rest,
        rest_other,
        values,
        opened,
        cum,
        rim,
    )
    pool = call(
        pool_kernel, shape((rows, cols), BF), [], 1 << 20, 1 << 19, info, pooled, before_pooled
    )
    part = call(
        final_kernel,
        shape((rows, width), BF),
        [
            *whole,
            pltpu.VMEM((rows, 2 * cols), BF),
            pltpu.VMEM((blocks[0], rows, width // blocks[0]), BF),
            pltpu.SemaphoreType.DMA((blocks[0],)),
        ],
        4 * rows * width * cols,
        8 << 20,
        info,
        start,
        growth,
        cum,
        decayed,
        heard,
        pool,
        out_gain[None, :],
        rest,
        rest_other,
        out_specs=HBM,
    )
    parts = lax.all_to_all(
        part.reshape(tp, rows // tp, width), "tp", split_axis=0, concat_axis=0, tiled=True
    )
    return jnp.sum(parts.astype(F32), axis=0).astype(BF)


def solution(mesh):
    split = Mesh(mesh.devices.reshape(4, 4, 4, 2, mesh.shape["tp"]), SP_TP)
    in_specs = (
        P(SP_TP, None),
        P(),
        P(SP, "tp"),
        P(SP, "tp"),
        P(SP, "tp"),
        P(SP, "tp"),
        P("tp"),
        P("tp", SP),
        P(),
        P("tp", SP),
        P("tp", SP),
    )
    out_specs = P(SP_TP, None)
    return jax.shard_map(layer, mesh=split, in_specs=in_specs, out_specs=out_specs, check_vma=False)
```
